32 devices in a mesh: grp: 1, ep: 16 (over z, y, x), tp: 2 (over core).
Axes of the slice: x: 2, y: 2, z: 4, core: 2. Of those that a mesh axis runs over, the one named last changes fastest.
Arguments:
- layer_input: bfloat16 [512, 2048], P(('grp', 'ep')), may hold values from -6 to 6
- ssm_state: float32 [2, 512, 32, 64], P(None, ('grp', 'ep'), 'tp'), may hold values from -4 to 4
- w_input: bfloat16 [2048, 512], P(None, 'tp'), may hold values from -0.125 to 0.125
- decay_rate: float32 [32, 64], P('tp'), may hold values from 0.05 to 2
- frequency: float32 [32, 64], P('tp'), may hold values from 0 to 20
- step_log: float32 [32], P('tp'), may hold values from -2.3 to 0
- input_map: float32 [2, 32, 64, 16], P(None, 'tp'), may hold values from -1 to 1
- output_map: float32 [2, 32, 16, 64], P(None, 'tp'), may hold values from -0.75 to 0.75
- skip_gain: float32 [32, 16], P('tp'), may hold values from -3 to 3
- glu_weight: bfloat16 [512, 512], replicated, may hold values from -0.25 to 0.25
- mix_out: bfloat16 [512, 2048], replicated, may hold values from -0.75 to 0.75
- norm_gain: float32 [2048], replicated, may hold values from 0.1 to 6, as said below
- norm_shift: float32 [2048], replicated, may hold values from -2 to 2
- route_ids: int32 [512, 6], P(('grp', 'ep')), may hold values from 0 to 15, all different within a row; in each aligned block of 32 rows (0 to 31, 32 to 63, ...) at most 24 rows name the same one
- route_weights: float32 [512, 6], P(('grp', 'ep')), may hold values from 0.1 to 1
- gate_expert: bfloat16 [16, 2048, 512], P('ep', None, 'tp'), may hold values from -0.125 to 0.125
- up_expert: bfloat16 [16, 2048, 512], P('ep', None, 'tp'), may hold values from -0.125 to 0.125
- down_expert: bfloat16 [16, 512, 2048], P('ep', 'tp'), may hold values from -0.25 to 0.25
- gate_shared: bfloat16 [2048, 512], P(None, 'tp'), may hold values from -0.125 to 0.125
- up_shared: bfloat16 [2048, 512], P(None, 'tp'), may hold values from -0.125 to 0.125
- down_shared: bfloat16 [512, 2048], P('tp'), may hold values from -0.25 to 0.25
- dense_in: bfloat16 [1024, 2048], P('ep'), may hold values from -0.125 to 0.125
- dense_out: bfloat16 [1024, 2048], P('ep', 'tp'), may hold values from -0.1875 to 0.1875
- branch_gate: bfloat16 [2048], replicated, may hold values from -0.125 to 0.125
- final_gain: float32 [2048], P('tp'), may hold values from 0.1 to 1.9
- final_shift: float32 [2048], P('tp'), may hold values from -2 to 2
Outputs:
- layer_output: bfloat16 [512, 2048], P(('grp', 'ep'), 'tp')
- new_state: float32 [2, 512, 32, 64], P(None, ('grp', 'ep'), 'tp')
The draws below stay inside these ranges and needn't reach their ends.
Inputs may be any that keep to these rules, and one draw needn't show every extreme that they name: `route_ids`: each row names 6 different experts; within each aligned block of 32 rows no expert is named more than 24 times, and in some block one expert is named exactly 24 times. `norm_gain`: positive gains.
All inputs are finite; a program needn't handle non-finite values.
Results may differ from the reference program's by a relative error of at most 0.015.
Values may be sent and summed in bfloat16 or wider, within the bound.
A program may use at most 128 MiB of HBM per device.

```python
import math
import jax
import jax.numpy as jnp
import numpy as np
from jax import lax

D = 2048
S5_WIDTH = 512
GROUP = 16
STATE = 64
EFF = 512
DENSE = 1024
TOP_K = 6
SEQ_DEV = 32
GROUPS = 32
EXPERTS = 16
SEQS = 512
CAP = 24
N_EP = 16
N_TP = 2


def draw_norm_gain(key, part):
    ramp = jnp.arange(D, dtype=jnp.float32) / D
    base = jnp.exp(math.log(0.3) + math.log(10.0) * ramp)
    noise = jax.random.uniform(jax.random.fold_in(key, 11), (D,), jnp.float32, 0.7, 1.3)
    return jnp.clip(base * noise, 0.1, 6.0).astype(jnp.float32)


def levels(own_key, dims, cuts, low, top_value):
    level = 1.0
    for axis_at, parts in cuts:
        draws = jax.random.uniform(jax.random.fold_in(jax.random.fold_in(own_key, 6), axis_at), (parts,), jnp.float32, low / len(cuts), top_value / len(cuts))
        level = level * jnp.repeat(jnp.exp(draws), dims[axis_at] // parts).reshape((-1,) + (1,) * (len(dims) - 1 - axis_at))
    return level


def routed_block(rng, own, number, rows, amount, top, reach, skew):
    order = jax.random.permutation(rng, amount)
    crowded, common = portions_of(amount, rows * top, reach, skew, True), portions_of(amount, rows * top, reach, skew, False)
    places = jnp.arange(amount)

    def named(lengths, turn):
        used = int((lengths > 0).sum())
        fixed = max(1, used // 4)
        passed = fixed + (places - fixed + turn * (used - fixed)) % max(1, amount - fixed)
        return jnp.zeros((amount,), jnp.int32).at[order[jnp.where(places < fixed, places, passed)]].set(jnp.asarray(lengths, jnp.int32))

    lengths = jnp.where(number % 4 == 0, named(crowded, number // 4), named(common, number - number // 4 - 1))
    mixed = jax.random.permutation(jax.random.fold_in(own, 3), amount)
    source_of, receiver = mixed[0:amount // 2 * 2:2], mixed[1:amount // 2 * 2:2]
    slack = jnp.minimum(lengths[source_of] - 1, reach - lengths[receiver]) // 2
    slack = jnp.where((source_of == order[0]) | (receiver == order[0]) | (lengths[receiver] == 0), 0, jnp.maximum(slack, 0))
    passed = jax.random.randint(jax.random.fold_in(own, 4), (amount // 2,), 0, 1 << 20) % (slack + 1)
    lengths = lengths.at[source_of].add(-passed).at[receiver].add(passed)
    members = jnp.searchsorted(jnp.cumsum(lengths), jnp.arange(rows * top), side="right").astype(jnp.int32)
    grid = members.reshape(top, rows).T
    grid = grid[jax.random.permutation(jax.random.fold_in(own, 1), rows)]
    turn = jax.random.randint(jax.random.fold_in(own, 2), (rows, 1), 0, top)
    return jnp.take_along_axis(grid, (jnp.arange(top)[None, :] + turn) % top, axis=1)


def portions_of(count, total, limit, skew, full):
    weights = [(1 << 20) // math.isqrt(rank ** skew) + 1 for rank in range(1, count + 1)]
    largest = limit if full else min(limit, max(-(-total // count), total * weights[0] // sum(weights)))
    least = 1 if total - largest >= count - 1 else 0
    counts, surplus = [largest] + [least] * (count - 1), total - largest - least * (count - 1)
    while surplus > 0:
        movable = [i for i in range(1, count) if counts[i] < largest] or [i for i in range(1, count) if counts[i] < limit]
        whole, budget = sum([weights[i] for i in movable]), surplus
        for i in movable:
            addition = min(limit - counts[i], max(1, budget * weights[i] // whole), surplus)
            counts[i] = counts[i] + addition
            surplus = surplus - addition
    return np.array(counts)


def scatter_about(key, dims, scale, most, cuts=(), kind=jnp.bfloat16):
    entries = jax.random.normal(key, dims, jnp.float32) * scale
    if len(cuts) > 0:
        entries = levels(key, dims, cuts, -0.22, 0.18) * entries
    return jnp.clip(entries, min=-most, max=most).astype(kind)


def setup_inputs(seed: int = 0, part: int = 0) -> dict:
    keys = jax.random.split(jax.random.key(seed), 27)
    own_keys = jax.random.split(jax.random.fold_in(keys[26], part), 27)
    layer_input = scatter_about(own_keys[0], (SEQS, D), 1.0, 6.0, ((0, 16),))
    ssm_state = scatter_about(own_keys[1], (2, SEQS, GROUPS, STATE), 0.5, 4.0, ((1, 16), (2, 2)), jnp.float32)
    w_input = scatter_about(keys[2], (D, S5_WIDTH), D ** -0.5, 0.125, ((1, 2),))
    decay_rate = jnp.clip(jnp.exp(math.log(2.0) - 3.6888794 * jax.random.uniform(keys[3], (GROUPS, STATE), jnp.float32) ** levels(keys[3], (GROUPS, STATE), ((0, 2),), -0.2, 0.2)), 0.05, 2.0)
    frequency = jnp.clip(20.0 * jax.random.uniform(keys[4], (GROUPS, STATE), jnp.float32) ** levels(keys[4], (GROUPS, STATE), ((0, 2),), -0.2, 0.2), 0.0, 20.0)
    step_log = jnp.clip(-2.3 + 2.3 * jax.random.uniform(keys[5], (GROUPS,), jnp.float32) ** levels(keys[5], (GROUPS,), ((0, 2),), -0.2, 0.2), -2.3, 0.0)
    input_map = scatter_about(keys[6], (2, GROUPS, STATE, GROUP), (2 * GROUP) ** -0.5, 1.0, ((1, 2),), jnp.float32)
    output_map = scatter_about(keys[7], (2, GROUPS, GROUP, STATE), STATE ** -0.5, 0.75, ((1, 2),), jnp.float32)
    skip_gain = scatter_about(keys[8], (GROUPS, GROUP), 0.5, 3.0, ((0, 2),), jnp.float32)
    glu_weight = scatter_about(keys[9], (S5_WIDTH, S5_WIDTH), S5_WIDTH ** -0.5, 0.25)
    mix_out = scatter_about(keys[10], (S5_WIDTH, D), (S5_WIDTH // 8) ** -0.5, 0.75)
    norm_gain = draw_norm_gain(jax.random.fold_in(keys[26], 71), part)
    norm_shift = scatter_about(keys[12], (D,), 0.3, 2.0, (), jnp.float32)
    route_ids_keys = jax.random.split(jax.random.fold_in(own_keys[13], 1), SEQS // SEQ_DEV)
    route_ids_turns = jax.random.permutation(jax.random.fold_in(own_keys[13], 3), SEQS // SEQ_DEV)
    route_ids = jax.vmap(lambda own, number: routed_block(jax.random.fold_in(own_keys[13], 2), own, number, SEQ_DEV, EXPERTS, TOP_K, CAP, 2))(route_ids_keys, route_ids_turns).reshape((SEQS, TOP_K))
    route_weights = jnp.clip(jnp.exp(math.log(1.0) - 2.3025851 * jax.random.uniform(own_keys[14], (SEQS, TOP_K), jnp.float32) ** levels(own_keys[14], (SEQS, TOP_K), ((0, 16),), -0.2, 0.2)), 0.1, 1.0)
    gate_expert = scatter_about(keys[15], (EXPERTS, D, EFF), D ** -0.5, 0.125, ((0, 16), (2, 2)))
    up_expert = scatter_about(keys[16], (EXPERTS, D, EFF), D ** -0.5, 0.125, ((0, 16), (2, 2)))
    down_expert = scatter_about(keys[17], (EXPERTS, EFF, D), EFF ** -0.5, 0.25, ((0, 16), (1, 2)))
    gate_shared = scatter_about(keys[18], (D, EFF), D ** -0.5, 0.125, ((1, 2),))
    up_shared = scatter_about(keys[19], (D, EFF), D ** -0.5, 0.125, ((1, 2),))
    down_shared = scatter_about(keys[20], (EFF, D), EFF ** -0.5, 0.25, ((0, 2),))
    dense_in = scatter_about(keys[21], (DENSE, D), D ** -0.5, 0.125, ((0, 16),))
    dense_out = scatter_about(keys[22], (DENSE, D), DENSE ** -0.5, 0.1875, ((0, 16), (1, 2)))
    branch_gate = scatter_about(keys[23], (D,), D ** -0.5, 0.125)
    final_gain = jnp.clip(1.0 + 0.18 * jax.random.normal(keys[24], (D,), jnp.float32), 0.1, 1.9)
    final_shift = scatter_about(keys[25], (D,), 0.3, 2.0, ((0, 2),), jnp.float32)
    return dict(layer_input=layer_input, ssm_state=ssm_state, w_input=w_input, decay_rate=decay_rate, frequency=frequency, step_log=step_log, input_map=input_map, output_map=output_map, skip_gain=skip_gain, glu_weight=glu_weight, mix_out=mix_out, norm_gain=norm_gain, norm_shift=norm_shift, route_ids=route_ids, route_weights=route_weights, gate_expert=gate_expert, up_expert=up_expert, down_expert=down_expert, gate_shared=gate_shared, up_shared=up_shared, down_shared=down_shared, dense_in=dense_in, dense_out=dense_out, branch_gate=branch_gate, final_gain=final_gain, final_shift=final_shift)


residual_alpha = 1.681792830507429
route_scale = 2.5
norm_eps = 1e-05
highest = lax.Precision.HIGHEST

def state_update(inputs, ssm_state, decay_rate, frequency, step_log, input_map, output_map, skip_gain):
    step_size = jnp.exp(step_log)[:, None]
    magnitude = jnp.exp(-decay_rate * step_size)
    rotation = frequency * step_size
    decay_re = magnitude * jnp.cos(rotation)
    decay_im = magnitude * jnp.sin(rotation)
    eigen_re = -decay_rate
    denominator = eigen_re * eigen_re + frequency * frequency
    factor_re = ((decay_re - 1.0) * eigen_re + decay_im * frequency) / denominator
    factor_im = (decay_im * eigen_re - (decay_re - 1.0) * frequency) / denominator
    drive_re = factor_re[..., None] * input_map[0] - factor_im[..., None] * input_map[1]
    drive_im = factor_re[..., None] * input_map[1] + factor_im[..., None] * input_map[0]
    pushed_re = jnp.einsum('gpm,tgm->tgp', drive_re, inputs, precision=highest)
    pushed_im = jnp.einsum('gpm,tgm->tgp', drive_im, inputs, precision=highest)
    new_re = decay_re * ssm_state[0] - decay_im * ssm_state[1] + pushed_re
    new_im = decay_re * ssm_state[1] + decay_im * ssm_state[0] + pushed_im
    response = jnp.einsum('gmp,tgp->tgm', output_map[0], new_re, precision=highest) - jnp.einsum('gmp,tgp->tgm', output_map[1], new_im, precision=highest) + skip_gain * inputs
    return (response, jnp.stack([new_re, new_im]))

def layer_norm_rows(values, gain, shift):
    mean = lax.optimization_barrier(jnp.mean(values, axis=1, keepdims=True))
    variance = lax.optimization_barrier(jnp.mean(jnp.square(values - mean), axis=1, keepdims=True))
    return (values - mean) * lax.rsqrt(variance + norm_eps) * gain + shift

def blockwise_down(hidden, down_weight):
    width = hidden.shape[1] // N_TP
    summed = jnp.zeros((hidden.shape[0], down_weight.shape[1]), jnp.float32)
    for portion in range(N_TP):
        part = jnp.dot(hidden[:, portion * width:(portion + 1) * width], down_weight[portion * width:(portion + 1) * width], preferred_element_type=jnp.float32)
        rounded = lax.optimization_barrier(part.astype(jnp.bfloat16))
        summed = summed + rounded.astype(jnp.float32)
    return summed.astype(jnp.bfloat16)

def swiglu_rows(rows, gate_weight, up_weight, down_weight):
    gate_part = jnp.dot(rows, gate_weight, preferred_element_type=jnp.float32)
    up_part = jnp.dot(rows, up_weight, preferred_element_type=jnp.float32)
    hidden = (jax.nn.silu(gate_part) * up_part).astype(jnp.bfloat16)
    return blockwise_down(hidden, down_weight)

def reference(layer_input, ssm_state, w_input, decay_rate, frequency, step_log, input_map, output_map, skip_gain, glu_weight, mix_out, norm_gain, norm_shift, route_ids, route_weights, gate_expert, up_expert, down_expert, gate_shared, up_shared, down_shared, dense_in, dense_out, branch_gate, final_gain, final_shift):
    projected = jnp.dot(layer_input, w_input, preferred_element_type=jnp.float32).astype(jnp.bfloat16)
    inputs = projected.astype(jnp.float32).reshape(SEQS, GROUPS, GROUP)
    response, new_state = state_update(inputs, ssm_state, decay_rate, frequency, step_log, input_map, output_map, skip_gain)
    activated = jax.nn.gelu(response.reshape(SEQS, S5_WIDTH)).astype(jnp.bfloat16)
    glu_out = (activated.astype(jnp.float32) * jax.nn.sigmoid(jnp.dot(activated, glu_weight, preferred_element_type=jnp.float32))).astype(jnp.bfloat16)
    mixed = jnp.dot(glu_out, mix_out, preferred_element_type=jnp.float32).astype(jnp.bfloat16)
    normed = layer_norm_rows(residual_alpha * layer_input.astype(jnp.float32) + mixed.astype(jnp.float32), norm_gain, norm_shift).astype(jnp.bfloat16)
    weights = route_weights / lax.optimization_barrier(jnp.sum(route_weights, axis=1, keepdims=True)) * route_scale
    choices_dev = SEQ_DEV * TOP_K
    block_ids = route_ids.reshape(N_EP, choices_dev)
    hits = (block_ids[..., None] == jnp.arange(EXPERTS, dtype=jnp.int32)).astype(jnp.int32)
    ranks = lax.optimization_barrier(jnp.sum((jnp.cumsum(hits, axis=1) - hits) * hits, axis=2)).astype(jnp.int32)
    sources = jnp.broadcast_to(jnp.arange(N_EP, dtype=jnp.int32)[:, None], (N_EP, choices_dev))
    repeated = jnp.repeat(normed.reshape(N_EP, SEQ_DEV, D), TOP_K, axis=1)
    buffer = jnp.zeros((N_EP, EXPERTS, CAP, D), jnp.bfloat16).at[sources, block_ids, ranks].set(repeated)
    per_expert = jnp.moveaxis(buffer, 1, 0)

    def run_expert(packed):
        slot_rows, gate_weight, up_weight, down_weight = packed
        result = swiglu_rows(slot_rows.reshape(N_EP * CAP, D), gate_weight, up_weight, down_weight)
        return result.reshape(N_EP, CAP, D)
    results = lax.map(run_expert, (per_expert, gate_expert, up_expert, down_expert))
    picked = results[block_ids, sources, ranks].astype(jnp.float32).reshape(SEQS, TOP_K, D)
    routed = lax.optimization_barrier(jnp.sum(picked * weights[:, :, None], axis=1))
    shared = swiglu_rows(normed, gate_shared, up_shared, down_shared)
    dense_hidden = jax.nn.gelu(jnp.dot(normed, dense_in.T, preferred_element_type=jnp.float32)).astype(jnp.bfloat16)
    dense = jnp.dot(dense_hidden, dense_out, preferred_element_type=jnp.float32)
    branch = jax.nn.sigmoid(jnp.dot(normed, branch_gate, preferred_element_type=jnp.float32))
    total = residual_alpha * normed.astype(jnp.float32) + routed + shared.astype(jnp.float32) + branch[:, None] * dense
    mean = lax.optimization_barrier(jnp.mean(total, axis=1, keepdims=True))
    variance = lax.optimization_barrier(jnp.mean(total * total, axis=1, keepdims=True)) - mean * mean
    layer_output = ((total - mean) * lax.rsqrt(variance + norm_eps) * final_gain + final_shift).astype(jnp.bfloat16)
    return (layer_output, new_state)
```

```python
import functools

import jax
import jax.numpy as jnp
from jax import lax
from jax.experimental import pallas as pl
from jax.experimental.pallas import tpu as pltpu
from jax.sharding import PartitionSpec as P

residual_alpha = 1.681792830507429
route_scale = 2.5
norm_eps = 1e-05
MESH = pl.DeviceIdType.MESH
f32 = jnp.float32
bf16 = jnp.bfloat16
NT = (((1,), (1,)), ((), ()))

bases = (0.0, 2.9, 5.8, 7.0, 9.8, 12.6, 15.6)
starts = (0.0, 5.0, 7.0, 9.0)
own_late = 9.0


def column(row, size):
    rows = lax.broadcasted_iota(jnp.int32, (size, size), 0)
    lanes = lax.broadcasted_iota(jnp.int32, (size, size), 1)
    return jnp.sum(jnp.where(rows == lanes, row, 0.0), axis=1, keepdims=True)


def layer_kernel(
    n_ep, local_experts,
    x_h, state_h, w_in_h, decay_h, freq_h, step_h, imap_h, omap_h, skip_h, glu_h, mix_h, ngain_h,
    nshift_h, ids_h, rw_h, gate_e, up_e, down_e, gate_s, up_s, down_s, dense_in, dense_out,
    bgate_h, fgain_h, fshift_h,
    out, state_out,
    xv, state, w_in, decay, freq, step, imap, omap, skip, glu, mix, ngain, nshift, ids, rw,
    bgate, fgain, fshift, push, pull, coef, new_state, act, nrm, wsend, wrecv,
    rows, wgu, wdo, wdx, sgu, sdo, sdx, din, dout,
    own, pbuf, precv, comb, rs1, s2buf, rs2, t3buf, t3recv, acc, sh_own, sh_oth, stat, statr,
    asem, wsem, ssem,
    route_s, route_r,
    line_s, line_r, one_s, one_r, twoa_s, twoa_r, twob_s, twob_r, da_s, da_r, db_s, db_r,
    p_s, p_r, fx_s, fx_r, fy_s, fy_r, rs2_s, rs2_r, t3_s, t3_r,
    act_s, act_r, stat_s, stat_r,
):
    nz = n_ep // 4
    R, width = xv.shape
    half = width // 2
    hid = gate_s.shape[1]
    ffn = gate_e.shape[2]
    dense_hid = dense_in.shape[0]
    chans = w_in.shape[1]
    groups, pst = decay.shape
    gch = chans // groups
    top_k = ids.shape[0]
    experts = n_ep * local_experts
    t = lax.axis_index("tp")
    e = lax.axis_index("ep")
    z = e // 4
    y = (e % 4) // 2
    x = e % 2
    a = y * (1 - t) + x * t
    b = x * (1 - t) + y * t
    ep_b = z * 4 + y * 2 + x + (1 - 2 * x) * (1 - t) + 2 * (1 - 2 * y) * t
    ep_a = z * 4 + y * 2 + x + (1 - 2 * x) * t + 2 * (1 - 2 * y) * (1 - t)
    yx = y * 2 + x

    def line_ep(other):
        return other * 4 + y * 2 + x

    mine = pl.ds(pl.multiple_of(t * half, half), half)
    peers = pl.ds(pl.multiple_of((1 - t) * half, half), half)

    barrier = pltpu.get_barrier_semaphore()
    pl.semaphore_signal(barrier, inc=1, device_id={"tp": 1 - t}, device_id_type=MESH)

    @pl.loop(1, n_ep)
    def _(k):
        pl.semaphore_signal(
            barrier, inc=1, device_id={"ep": (e + k) % n_ep}, device_id_type=MESH
        )

    first_loads = [
        (step_h, step), (decay_h, decay), (freq_h, freq), (imap_h, imap), (omap_h, omap),
        (skip_h, skip), (x_h, xv), (w_in_h, w_in), (ids_h, ids), (rw_h, rw), (state_h, state),
        (ngain_h, ngain), (nshift_h, nshift), (glu_h, glu), (mix_h, mix),
    ]
    loads_a = [
        pltpu.make_async_copy(s, d, asem.at[i]) for i, (s, d) in enumerate(first_loads)
    ]
    shared_copies = [
        (gate_s, sgu.at[:, pl.ds(0, hid)]),
        (up_s, sgu.at[:, pl.ds(hid, hid)]),
        (down_s.at[:, mine], sdo),
        (down_s.at[:, peers], sdx),
    ]
    expert_copies = []
    for l in range(local_experts):
        expert_copies += [
            (gate_e.at[l], wgu.at[l, :, pl.ds(0, ffn)]),
            (up_e.at[l], wgu.at[l, :, pl.ds(ffn, ffn)]),
            (down_e.at[l, :, mine], wdo.at[l]),
            (down_e.at[l, :, peers], wdx.at[l]),
        ]
    expert_copies += [
        (dense_in, din.at[pl.ds(0, dense_hid)]),
        (dense_out, dout),
        (bgate_h, bgate),
        (fgain_h, fgain),
        (fshift_h, fshift),
    ]
    loads_b = [
        pltpu.make_async_copy(s, d, wsem.at[i])
        for i, (s, d) in enumerate(shared_copies + expert_copies)
    ]
    for c in loads_a[:13]:
        c.start()

    def remote(src, dst, ss, rs, where):
        return pltpu.make_async_remote_copy(
            src_ref=src, dst_ref=dst, send_sem=ss, recv_sem=rs,
            device_id=where, device_id_type=MESH,
        )

    def event(s):
        s = s if isinstance(s, int) and s == 0 else nz - s
        if isinstance(s, int) and s == 0:
            return z
        m = jnp.minimum(z, nz - 1 - z)
        k = (s + 1) // 2
        near = jnp.where(s % 2 == 1, z - k, z + k)
        far = jnp.where(z <= nz - 1 - z, s, nz - 1 - s)
        return jnp.where(s <= 2 * m, near, far)

    def route(other):
        return remote(wsend.at[other], wrecv.at[e], route_s.at[other], route_r.at[e],
                      {"ep": other})

    def route_wait(other):
        remote(wsend.at[other], wrecv.at[other], route_s.at[other], route_r.at[other],
               {"ep": other}).wait_recv()

    def line_copy(other):
        return remote(rows.at[t, z, a, b], rows.at[t, z, a, b], line_s.at[other], line_r.at[z],
                      {"ep": line_ep(other)})

    def line_wait(j):
        remote(rows.at[t, j, a, b], rows.at[t, j, a, b], line_s.at[j], line_r.at[j],
               {"ep": line_ep(j)}).wait_recv()

    def one(j, at):
        return remote(rows.at[t, j, a, at], rows.at[t, j, a, at], one_s.at[j], one_r.at[j],
                      {"ep": ep_b})

    def twoa(j, at):
        return remote(rows.at[t, j, at, b], rows.at[t, j, at, b], twoa_s.at[j], twoa_r.at[j],
                      {"ep": ep_a})

    def twob(j, at):
        return remote(rows.at[t, j, at, 1 - b], rows.at[t, j, at, 1 - b], twob_s.at[j],
                      twob_r.at[j], {"ep": ep_a})

    def da(j):
        return remote(rows.at[t, j, a], rows.at[t, j, a], da_s.at[j], da_r.at[j], {"tp": 1 - t})

    def da_wait(j):
        remote(rows.at[1 - t, j, b], rows.at[1 - t, j, b], da_s.at[j], da_r.at[j],
               {"tp": 1 - t}).wait_recv()

    def db(j):
        return remote(rows.at[t, j, 1 - a], rows.at[t, j, 1 - a], db_s.at[j], db_r.at[j],
                      {"tp": 1 - t})

    def db_wait(j):
        remote(rows.at[1 - t, j, 1 - b], rows.at[1 - t, j, 1 - b], db_s.at[j], db_r.at[j],
               {"tp": 1 - t}).wait_recv()

    def part(j):
        return remote(pbuf.at[j], precv.at[j], p_s.at[j], p_r.at[j], {"tp": 1 - t})

    def firstx(j):
        return remote(comb.at[j, 1 - a, 1 - b], rs1.at[j, 1 - b], fx_s.at[j], fx_r.at[j],
                      {"ep": ep_a})

    def firsty(j):
        return remote(comb.at[j, 1 - a, b], rs1.at[j, b], fy_s.at[j], fy_r.at[j],
                      {"ep": ep_a})

    def second(j):
        return remote(s2buf.at[j], rs2.at[j], rs2_s.at[j], rs2_r.at[j], {"ep": ep_b})

    def third(j):
        return remote(t3buf.at[j], t3recv.at[z], t3_s.at[j], t3_r.at[z], {"ep": line_ep(j)})

    def third_wait(j):
        remote(t3buf.at[j], t3recv.at[j], t3_s.at[j], t3_r.at[j],
               {"ep": line_ep(j)}).wait_recv()

    push[...] = jnp.zeros(push.shape, bf16)
    pull[...] = jnp.zeros(pull.shape, bf16)
    wsend[...] = jnp.zeros(wsend.shape, f32)
    din[pl.ds(dense_hid, din.shape[0] - dense_hid), :] = jnp.zeros(
        (din.shape[0] - dense_hid, width), bf16
    )
    for c in loads_a[:6]:
        c.wait()
    for c in loads_a[13:]:
        c.start()
    size = column(jnp.exp(step[...]), groups)
    rate = decay[...]
    turn = freq[...]
    magnitude = jnp.exp(-rate * size)
    rotation = turn * size
    decay_re = magnitude * jnp.cos(rotation)
    decay_im = magnitude * jnp.sin(rotation)
    denominator = rate * rate + turn * turn
    coef[0] = decay_re
    coef[1] = decay_im
    coef[2] = (decay_im * turn - (decay_re - 1.0) * rate) / denominator
    coef[3] = (-decay_im * rate - (decay_re - 1.0) * turn) / denominator
    spread = (
        lax.broadcasted_iota(jnp.int32, (gch, chans), 1) % gch
        == lax.broadcasted_iota(jnp.int32, (gch, chans), 0)
    ).astype(f32)
    tiled = jnp.dot(
        skip[...], spread, precision=lax.Precision.HIGHEST, preferred_element_type=f32
    )
    picked = (
        lax.broadcasted_iota(jnp.int32, (groups, chans), 1) // gch
        == lax.broadcasted_iota(jnp.int32, (groups, chans), 0)
    )
    skip_row = jnp.sum(jnp.where(picked, tiled, 0.0), axis=0, keepdims=True)
    lump = 128 // gch
    lumps = chans // 128
    for g in range(groups):
        h, k = g // lump, g % lump
        at = pl.ds(k * gch, gch)
        lanes = pl.ds(k * 2 * pst, 2 * pst)
        src = pl.ds(g * gch, gch)
        push[h, at, lanes] = jnp.concatenate([imap[0, src], imap[1, src]], axis=1).astype(bf16)
        pull[h, at, lanes] = jnp.concatenate([omap[0, src], -omap[1, src]], axis=1).astype(bf16)
    loads_a[6].wait()
    loads_a[7].wait()
    projected = jnp.dot(xv[...], w_in[...], preferred_element_type=f32).astype(bf16)
    loads_a[8].wait()
    loads_a[9].wait()
    scores = rw[...]
    scores = scores / jnp.sum(scores, axis=0, keepdims=True) * route_scale
    expert = lax.broadcasted_iota(jnp.int32, (experts, R), 0)
    table = jnp.zeros((experts, R), f32)
    for k in range(top_k):
        table += jnp.where(ids[k:k + 1, :] == expert, scores[k:k + 1, :], 0.0)
    for o in range(n_ep):
        wsend[o, pl.ds(0, local_experts), pl.ds(0, R)] = table[
            o * local_experts:(o + 1) * local_experts
        ]
    wrecv[e] = wsend[e]
    loads_a[10].wait()
    responses = []
    for h in range(lumps):
        pushed = jnp.dot(
            projected[:, h * 128:(h + 1) * 128], push[h], preferred_element_type=f32
        )
        fresh = []
        for k in range(lump):
            g = h * lump + k
            u = pushed[:, k * 2 * pst:k * 2 * pst + pst]
            v = pushed[:, k * 2 * pst + pst:(k + 1) * 2 * pst]
            old_re = state[pl.ds(g, R, stride=groups), :]
            old_im = state[pl.ds(R * groups + g, R, stride=groups), :]
            dr = coef[0, g:g + 1, :]
            di = coef[1, g:g + 1, :]
            fr = coef[2, g:g + 1, :]
            fi = coef[3, g:g + 1, :]
            new_re = dr * old_re - di * old_im + fr * u - fi * v
            new_im = dr * old_im + di * old_re + fr * v + fi * u
            new_state[pl.ds(g, R, stride=groups), :] = new_re
            new_state[pl.ds(R * groups + g, R, stride=groups), :] = new_im
            fresh += [new_re, new_im]
        fresh = jnp.concatenate(fresh, axis=1).astype(bf16)
        responses.append(lax.dot_general(fresh, pull[h], NT, preferred_element_type=f32))
    response = jnp.concatenate(responses, axis=1) + skip_row * projected.astype(f32)
    act[t] = jax.nn.gelu(response).astype(bf16)
    keep_state = pltpu.make_async_copy(new_state, state_out, ssem)
    pl.semaphore_wait(barrier, n_ep)
    swap = remote(act.at[t], act.at[t], act_s, act_r, {"tp": 1 - t})
    swap.start()
    for c in loads_b:
        c.start()
    keep_state.start()

    @pl.loop(1, n_ep)
    def _(k):
        route((e + k) % n_ep).start()

    loads_a[13].wait()
    logits = jnp.dot(
        act[t], glu[pl.ds(pl.multiple_of(t * chans, chans), chans), :],
        preferred_element_type=f32,
    )
    loads_a[14].wait()
    loads_a[11].wait()
    loads_a[12].wait()
    remote(act.at[1 - t], act.at[1 - t], act_s, act_r, {"tp": 1 - t}).wait_recv()
    logits += jnp.dot(
        act[1 - t], glu[pl.ds(pl.multiple_of((1 - t) * chans, chans), chans), :],
        preferred_element_type=f32,
    )
    every = jnp.concatenate([act[0], act[1]], axis=1)
    glu_out = (every.astype(f32) * jax.nn.sigmoid(logits)).astype(bf16)
    mixed = jnp.dot(glu_out, mix[...], preferred_element_type=f32).astype(bf16)
    values = residual_alpha * xv[...].astype(f32) + mixed.astype(f32)
    values = values - jnp.mean(values, axis=1, keepdims=True)
    variance = jnp.mean(jnp.square(values), axis=1, keepdims=True)
    nrm[...] = (values * lax.rsqrt(variance + norm_eps) * ngain[...] + nshift[...]).astype(bf16)
    rows[t, z, a, b] = nrm[:, mine]

    @pl.loop(1, nz)
    def _(s):
        line_copy(event(s)).start()

    one(z, b).start()
    twoa(z, a).start()

    for c in loads_b[:4]:
        c.wait()
    gu = jnp.dot(nrm[...], sgu[...], preferred_element_type=f32)
    sh = (jax.nn.silu(gu[:, :hid]) * gu[:, hid:]).astype(bf16)
    sh_own[...] = jnp.dot(sh, sdo[...], preferred_element_type=f32)
    sh_oth[...] = jnp.dot(sh, sdx[...], preferred_element_type=f32)
    for c in loads_b[4:]:
        c.wait()
    din[pl.ds(dense_hid, 1), :] = bgate[...]

    @pl.loop(1, n_ep)
    def _(k):
        route_wait((e + k) % n_ep)

    def place(k):
        yy, xx = k // 2, k % 2
        return yy * (1 - t) + xx * t, xx * (1 - t) + yy * t

    def compute(s, j):
        x0 = jnp.concatenate([rows[0, j, k // 2, k % 2] for k in range(4)], axis=0)
        x1 = jnp.concatenate([rows[1, j, k % 2, k // 2] for k in range(4)], axis=0)
        hidden = []
        oth_part = None
        for l in range(local_experts):
            w = jnp.concatenate(
                [column(wrecv[j * 4 + k, l:l + 1, 0:R], R) for k in range(4)], axis=0
            )
            g = jnp.dot(x0, wgu[l, :half], preferred_element_type=f32)
            g += jnp.dot(x1, wgu[l, half:], preferred_element_type=f32)
            h = (jax.nn.silu(g[:, :ffn]) * g[:, ffn:] * w).astype(bf16)
            hidden.append(h)
            o = jnp.dot(h, wdx[l], preferred_element_type=f32)
            oth_part = o if oth_part is None else oth_part + o
        pbuf[j] = oth_part.astype(bf16).reshape(4, R, half)

        if s == 0:
            pbuf[j, yx] = (pbuf[j, yx].astype(f32) + sh_oth[...]).astype(bf16)
        part(j).start()
        d = lax.dot_general(x0, din[:, :half], NT, preferred_element_type=f32)
        d += lax.dot_general(x1, din[:, half:], NT, preferred_element_type=f32)
        branch = jax.nn.sigmoid(d[:, dense_hid:dense_hid + 1])
        dh = (jax.nn.gelu(d[:, :dense_hid]) * branch).astype(bf16)
        own_part = jnp.dot(dh, dout[...], preferred_element_type=f32)
        for l in range(local_experts):
            own_part += jnp.dot(hidden[l], wdo[l], preferred_element_type=f32)
        own[j] = own_part.reshape(4, R, half)

    def stage_a(s, j):
        if s > 0:
            line_wait(j)
            one(j, b).start()
            twoa(j, a).start()

    def stage_b(s, j):
        one(j, 1 - b).wait_recv()
        twob(j, a).start()
        da(j).start()

    def stage_c(s, j):
        twoa(j, 1 - a).wait_recv()
        twob(j, 1 - a).wait_recv()
        db(j).start()

    def stage_d(s, j):
        da_wait(j)
        db_wait(j)
        compute(s, j)

    def stage_e(s, j):
        part(j).wait_recv()
        for k in range(4):
            aa, bb = place(k)
            comb[j, aa, bb] = (own[j, k] + precv[j, k].astype(f32)).astype(bf16)
        firstx(j).start()
        firsty(j).start()

    def stage_f(s, j):
        remote(comb.at[j, 1 - a, 1 - b], rs1.at[j, 1 - b], fx_s.at[j], fx_r.at[j],
               {"ep": ep_a}).wait_recv()
        s2buf[j] = (comb[j, a, 1 - b].astype(f32) + rs1[j, 1 - b].astype(f32)).astype(bf16)
        second(j).start()

    def stage_g(s, j):
        firsty(j).wait_recv()
        second(j).wait_recv()
        summed = comb[j, a, b].astype(f32) + rs1[j, b].astype(f32) + rs2[j].astype(f32)

        if s == 0:
            acc[...] = summed + sh_own[...] + residual_alpha * nrm[:, mine].astype(f32)
        else:
            t3buf[j] = summed.astype(bf16)
            third(j).start()

    runs = (stage_a, stage_b, stage_c, stage_d, stage_e, stage_f, stage_g)

    def when(i, s):
        start = starts[s] if s < len(starts) else starts[-1] + 2.0 * (s - len(starts) + 1)
        late = own_late if s == 0 and i >= 4 else 0.0
        return bases[i] + start + late

    plan = sorted((when(i, s), i, s) for i in range(7) for s in range(nz))
    for _, i, s in plan:
        runs[i](s, event(s))

    @pl.loop(1, nz)
    def _(s):
        j = event(s)
        third_wait(j)
        acc[...] += t3recv[j].astype(f32)

    total = acc[...]
    lane = lax.broadcasted_iota(jnp.int32, stat.shape, 1)
    row_sum = jnp.sum(total, axis=1, keepdims=True)
    row_sq = jnp.sum(total * total, axis=1, keepdims=True)
    stat[...] = jnp.where(lane == 0, row_sum, row_sq)
    exchange = remote(stat, statr, stat_s, stat_r, {"tp": 1 - t})
    exchange.start()
    swap.wait_send()
    keep_state.wait()

    @pl.loop(1, n_ep)
    def _(k):
        route((e + k) % n_ep).wait_send()

    @pl.loop(0, nz)
    def _(j):
        one(j, b).wait_send()
        twoa(j, a).wait_send()
        twob(j, a).wait_send()
        da(j).wait_send()
        db(j).wait_send()
        part(j).wait_send()
        firstx(j).wait_send()
        firsty(j).wait_send()
        second(j).wait_send()

    @pl.loop(1, nz)
    def _(s):
        j = event(s)
        line_copy(j).wait_send()
        third(j).wait_send()

    exchange.wait()
    mean = (row_sum + statr[:, 0:1]) / width
    variance = (row_sq + statr[:, 1:2]) / width - mean * mean
    out[...] = (
        (total - mean) * lax.rsqrt(variance + norm_eps) * fgain[...] + fshift[...]
    ).astype(bf16)


def body(
    layer_input, ssm_state, w_input, decay_rate, frequency, step_log, input_map, output_map,
    skip_gain, glu_weight, mix_out, norm_gain, norm_shift, route_ids, route_weights,
    gate_expert, up_expert, down_expert, gate_shared, up_shared, down_shared,
    dense_in, dense_out, branch_gate, final_gain, final_shift,
):
    n_ep = lax.axis_size("ep")
    R, width = layer_input.shape
    half = width // 2
    local_experts, _, ffn = gate_expert.shape
    hid = gate_shared.shape[1]
    dense_hid = dense_in.shape[0]
    groups, gch = skip_gain.shape
    pst = decay_rate.shape[1]
    chans = groups * gch
    top_k = route_ids.shape[1]
    nz = n_ep // 4
    lumps = chans // 128
    wide = (128 // gch) * 2 * pst
    dense_pad = -(-(dense_hid + 1) // 128) * 128
    exp_pad = -(-local_experts // 8) * 8
    operands = (
        layer_input,
        ssm_state.reshape(2 * R * groups, pst),
        w_input,
        decay_rate,
        frequency,
        step_log[None, :],
        input_map.transpose(0, 1, 3, 2).reshape(2, chans, pst),
        output_map.reshape(2, chans, pst),
        skip_gain,
        glu_weight,
        mix_out,
        norm_gain[None, :],
        norm_shift[None, :],
        route_ids.T,
        route_weights.T,
        gate_expert, up_expert, down_expert, gate_shared, up_shared, down_shared,
        dense_in, dense_out,
        branch_gate[None, :],
        final_gain[None, :],
        final_shift[None, :],
    )
    hbm = pl.BlockSpec(memory_space=pl.ANY)
    vmem = pl.BlockSpec(memory_space=pltpu.VMEM)
    dma = pltpu.SemaphoreType.DMA

    def like(i):
        return pltpu.VMEM(operands[i].shape, operands[i].dtype)

    layer_output, new_state = pl.pallas_call(
        functools.partial(layer_kernel, n_ep, local_experts),
        out_shape=(
            jax.ShapeDtypeStruct((R, half), bf16),
            jax.ShapeDtypeStruct((2 * R * groups, pst), f32),
        ),
        in_specs=[hbm] * len(operands),
        out_specs=(vmem, hbm),
        scratch_shapes=[like(i) for i in range(15)]
        + [like(i) for i in (23, 24, 25)]
        + [
            pltpu.VMEM((lumps, 128, wide), bf16),
            pltpu.VMEM((lumps, 128, wide), bf16),
            pltpu.VMEM((4, groups, pst), f32),
            pltpu.VMEM((2 * R * groups, pst), f32),
            pltpu.VMEM((2, R, chans), bf16),
            pltpu.VMEM((R, width), bf16),
            pltpu.VMEM((n_ep, exp_pad, 128), f32),
            pltpu.VMEM((n_ep, exp_pad, 128), f32),
            pltpu.VMEM((2, nz, 2, 2, R, half), bf16),
            pltpu.VMEM((local_experts, width, 2 * ffn), bf16),
            pltpu.VMEM((local_experts, ffn, half), bf16),
            pltpu.VMEM((local_experts, ffn, half), bf16),
            pltpu.VMEM((width, 2 * hid), bf16),
            pltpu.VMEM((hid, half), bf16),
            pltpu.VMEM((hid, half), bf16),
            pltpu.VMEM((dense_pad, width), bf16),
            pltpu.VMEM((dense_hid, half), bf16),
            pltpu.VMEM((nz, 4, R, half), f32),
            pltpu.VMEM((nz, 4, R, half), bf16),
            pltpu.VMEM((nz, 4, R, half), bf16),
            pltpu.VMEM((nz, 2, 2, R, half), bf16),
            pltpu.VMEM((nz, 2, R, half), bf16),
            pltpu.VMEM((nz, R, half), bf16),
            pltpu.VMEM((nz, R, half), bf16),
            pltpu.VMEM((nz, R, half), bf16),
            pltpu.VMEM((nz, R, half), bf16),
            pltpu.VMEM((R, half), f32),
            pltpu.VMEM((R, half), f32),
            pltpu.VMEM((R, half), f32),
            pltpu.VMEM((R, 128), f32),
            pltpu.VMEM((R, 128), f32),
            dma((15,)),
            dma((9 + 4 * local_experts,)),
            dma,
            dma((n_ep,)),
            dma((n_ep,)),
        ]
        + [dma((nz,))] * 22
        + [dma] * 4,
        compiler_params=pltpu.CompilerParams(
            collective_id=0, has_side_effects=True, vmem_limit_bytes=60 * 1024 * 1024
        ),
    )(*operands)
    return (layer_output, new_state.reshape(2, R, groups, pst))


def solution(mesh):
    placed = (
        P(("grp", "ep"), None),
        P(None, ("grp", "ep"), "tp", None),
        P(None, "tp"),
        P("tp", None),
        P("tp", None),
        P("tp"),
        P(None, "tp", None, None),
        P(None, "tp", None, None),
        P("tp", None),
        P(),
        P(),
        P(),
        P(),
        P(("grp", "ep"), None),
        P(("grp", "ep"), None),
        P("ep", None, "tp"),
        P("ep", None, "tp"),
        P("ep", "tp", None),
        P(None, "tp"),
        P(None, "tp"),
        P("tp", None),
        P("ep", None),
        P("ep", "tp"),
        P(),
        P("tp"),
        P("tp"),
    )
    return jax.shard_map(
        body,
        mesh=mesh,
        in_specs=placed,
        out_specs=(P(("grp", "ep"), "tp"), P(None, ("grp", "ep"), "tp", None)),
        check_vma=False,
    )
```

```python
import functools

import jax
import jax.numpy as jnp
from jax import lax
from jax.experimental import pallas as pl
from jax.experimental.pallas import tpu as pltpu
from jax.sharding import PartitionSpec as P

residual_alpha = 1.681792830507429
route_scale = 2.5
norm_eps = 1e-05
MESH = pl.DeviceIdType.MESH
f32 = jnp.float32
bf16 = jnp.bfloat16
NT = (((1,), (1,)), ((), ()))

order = (
    "H", "B0", "A1", "A2", "C0", "P0", "T1", "A3", "B1", "B2", "T2", "Q0", "T3", "C1", "R0",
    "E0", "P1", "B3", "Y0", "Q1", "C2", "R1", "P2", "E1", "Y1", "Q2", "C3", "F0", "P3", "R2",
    "E2", "Q3", "F1", "R3", "E3", "F2", "Y2", "G1", "Y3", "F3", "G2", "G0", "G3",
)


def column(row, size):
    rows = lax.broadcasted_iota(jnp.int32, (size, size), 0)
    lanes = lax.broadcasted_iota(jnp.int32, (size, size), 1)
    return jnp.sum(jnp.where(rows == lanes, row, 0.0), axis=1, keepdims=True)


def layer_kernel(
    n_ep, local_experts,
    x_h, state_h, w_in_h, decay_h, freq_h, step_h, imap_h, omap_h, skip_h, glu_h, mix_h, ngain_h,
    nshift_h, ids_h, rw_h, gate_e, up_e, down_e, gate_s, up_s, down_s, dense_in, dense_out,
    bgate_h, fgain_h, fshift_h,
    out, new_state,
    xv, state, w_in, decay, freq, step, imap, omap, skip, glu, mix, ngain, nshift, ids, rw,
    bgate, fnorm, push, pull, coef, moved, act, nrm, wsend, wrecv,
    rows, wgu, wd, sgu, sd, din, dout,
    own, gacc, dacc, hbuf, pbuf, precv, comb, rs1, s2buf, rs2, t3buf, t3recv, acc, sh_own, sh_oth, stat, statr,
    asem, wsem,
    route_s, route_r,
    line_r, one_r, two_r, d_r, p_r, fx_r, g_r,
    t3_r, line_s, one_s, twoa_s, twob_s, da_s, db_s, p_s, fx_s, fy_s, rs2_s, t3_s,
    act_s, act_r, stat_s, stat_r,
):
    nz = n_ep // 4
    R, width = xv.shape
    half = width // 2
    hid = gate_s.shape[1]
    ffn = gate_e.shape[2]
    dense_hid = dense_in.shape[0]
    chans = w_in.shape[1]
    groups, pst = decay.shape
    gch = chans // groups
    top_k = ids.shape[0]
    experts = n_ep * local_experts
    t = lax.axis_index("tp")
    e = lax.axis_index("ep")
    z = e // 4
    y = (e % 4) // 2
    x = e % 2
    a = y * (1 - t) + x * t
    b = x * (1 - t) + y * t
    ep_b = z * 4 + y * 2 + x + (1 - 2 * x) * (1 - t) + 2 * (1 - 2 * y) * t
    ep_a = z * 4 + y * 2 + x + (1 - 2 * x) * t + 2 * (1 - 2 * y) * (1 - t)

    def line_ep(other):
        return other * 4 + y * 2 + x

    mine = pl.ds(pl.multiple_of(t * half, half), half)
    peers = pl.ds(pl.multiple_of((1 - t) * half, half), half)

    first_loads = [
        (step_h, step), (decay_h, decay), (freq_h, freq), (imap_h, imap), (omap_h, omap),
        (skip_h, skip), (x_h, xv), (w_in_h, w_in), (ids_h, ids), (rw_h, rw), (state_h, state),
        (ngain_h, ngain), (nshift_h, nshift), (glu_h, glu), (mix_h, mix),
    ]
    loads_a = [
        pltpu.make_async_copy(s, d, asem.at[i]) for i, (s, d) in enumerate(first_loads)
    ]
    fetch = [
        (gate_s, sgu.at[:, pl.ds(0, hid)], 0),
        (up_s, sgu.at[:, pl.ds(hid, hid)], 0),
        (down_s, sd, 1),
    ]
    for l in range(local_experts):
        fetch += [
            (gate_e.at[l], wgu.at[l, :, pl.ds(0, ffn)], 2),
            (up_e.at[l], wgu.at[l, :, pl.ds(ffn, ffn)], 2),
        ]
    fetch += [
        (down_e, wd, 3),
        (dense_in, din.at[pl.ds(0, dense_hid)], 4),
        (dense_out, dout, 5),
        (bgate_h, bgate, 6),
        (fgain_h, fnorm.at[0:1], 7),
        (fshift_h, fnorm.at[1:2], 7),
    ]
    loads_b = [pltpu.make_async_copy(src, dst, wsem.at[i]) for src, dst, i in fetch]

    def fetched(ref, i):
        pltpu.make_async_copy(ref, ref, wsem.at[i]).wait()

    for i in (7, 6, 5, 4, 3, 2, 1, 0, 10, 8, 9, 11, 12):
        loads_a[i].start()

    barrier = pltpu.get_barrier_semaphore()
    pl.semaphore_signal(barrier, inc=1, device_id={"tp": 1 - t}, device_id_type=MESH)

    @pl.loop(1, n_ep)
    def _(k):
        pl.semaphore_signal(
            barrier, inc=1, device_id={"ep": (e + k) % n_ep}, device_id_type=MESH
        )

    def remote(src, dst, ss, rs, where):
        return pltpu.make_async_remote_copy(
            src_ref=src, dst_ref=dst, send_sem=ss, recv_sem=rs,
            device_id=where, device_id_type=MESH,
        )

    def event(s):
        if isinstance(s, int) and s == 0:
            return z
        return jnp.where(s - 1 >= z, s, s - 1)

    def route(other):
        return remote(wsend.at[other], wrecv.at[e], route_s, route_r, {"ep": other})

    def routes():
        most = pl.ds(0, n_ep - 1)
        return remote(wsend.at[most], wrecv.at[most], route_s, route_r, {"ep": (e + 1) % n_ep})

    def line_copy(other):
        return remote(rows.at[t, z, a, b], rows.at[t, z, a, b], line_s, line_r.at[z],
                      {"ep": line_ep(other)})

    def line_wait(j):
        remote(rows.at[t, j, a, b], rows.at[t, j, a, b], line_s, line_r.at[j],
               {"ep": ep_a}).wait_recv()

    def one(j, at):
        return remote(rows.at[t, j, a, at], rows.at[t, j, a, at], one_s, one_r.at[j],
                      {"ep": ep_b})

    def twoa(j):
        return remote(rows.at[t, j, a, b], rows.at[t, j, a, b], twoa_s, two_r.at[j],
                      {"ep": ep_a})

    def twob(j):
        return remote(rows.at[t, j, a, 1 - b], rows.at[t, j, a, 1 - b], twob_s, two_r.at[j],
                      {"ep": ep_a})

    def two_wait(j):
        remote(rows.at[t, j, 1 - a], rows.at[t, j, 1 - a], twoa_s, two_r.at[j],
               {"ep": ep_a}).wait_recv()

    def da(j):
        return remote(rows.at[t, j, a], rows.at[t, j, a], da_s, d_r.at[j], {"tp": 1 - t})

    def db(j):
        return remote(rows.at[t, j, 1 - a], rows.at[t, j, 1 - a], db_s, d_r.at[j],
                      {"tp": 1 - t})

    def d_wait(j):
        remote(rows.at[1 - t, j], rows.at[1 - t, j], da_s, d_r.at[j], {"tp": 1 - t}).wait_recv()

    def part(j):
        return remote(pbuf.at[j], precv.at[j], p_s, p_r.at[j], {"tp": 1 - t})

    def firstx(j):
        return remote(comb.at[j, 1 - a, 1 - b], rs1.at[j, 1 - b], fx_s, fx_r.at[j],
                      {"ep": ep_a})

    def firsty(j):
        return remote(comb.at[j, 1 - a, b], rs1.at[j, b], fy_s, g_r.at[j], {"ep": ep_a})

    def second(j):
        return remote(s2buf.at[j], rs2.at[j], rs2_s, g_r.at[j], {"ep": ep_b})

    def g_wait(j):
        remote(rs1.at[j], rs1.at[j], rs2_s, g_r.at[j], {"ep": ep_b}).wait_recv()

    def third(j):
        return remote(t3buf.at[j], t3recv.at[z], t3_s, t3_r, {"ep": line_ep(j)})

    lines = pl.ds(0, nz - 1)

    def thirds():
        return remote(t3buf.at[lines], t3recv.at[lines], t3_s, t3_r, {"ep": ep_a})

    def sent(ref, sem):
        remote(ref, ref, sem, t3_r, {"ep": ep_a}).wait_send()

    push[...] = jnp.zeros(push.shape, bf16)
    pull[...] = jnp.zeros(pull.shape, bf16)
    wsend[...] = jnp.zeros(wsend.shape, f32)
    din[pl.ds(dense_hid, din.shape[0] - dense_hid), :] = jnp.zeros(
        (din.shape[0] - dense_hid, width), bf16
    )
    for c in loads_a[:6]:
        c.wait()
    for c in loads_a[13:]:
        c.start()
    size = column(jnp.exp(step[...]), groups)
    rate = decay[...]
    turn = freq[...]
    magnitude = jnp.exp(-rate * size)
    rotation = turn * size
    decay_re = magnitude * jnp.cos(rotation)
    decay_im = magnitude * jnp.sin(rotation)
    denominator = rate * rate + turn * turn
    factor_re = (decay_im * turn - (decay_re - 1.0) * rate) / denominator
    factor_im = (-decay_im * rate - (decay_re - 1.0) * turn) / denominator
    coef[0] = jnp.concatenate([decay_re, decay_re], axis=1)
    coef[1] = jnp.concatenate([-decay_im, decay_im], axis=1)
    coef[2] = jnp.concatenate([factor_re, factor_re], axis=1)
    coef[3] = jnp.concatenate([-factor_im, factor_im], axis=1)
    spread = (
        lax.broadcasted_iota(jnp.int32, (gch, chans), 1) % gch
        == lax.broadcasted_iota(jnp.int32, (gch, chans), 0)
    ).astype(f32)
    tiled = jnp.dot(
        skip[...], spread, precision=lax.Precision.HIGHEST, preferred_element_type=f32
    )
    picked = (
        lax.broadcasted_iota(jnp.int32, (groups, chans), 1) // gch
        == lax.broadcasted_iota(jnp.int32, (groups, chans), 0)
    )
    skip_row = jnp.sum(jnp.where(picked, tiled, 0.0), axis=0, keepdims=True)
    lump = 128 // gch
    lumps = chans // 128
    for g in range(groups):
        h, k = g // lump, g % lump
        at = pl.ds(k * gch, gch)
        lanes = pl.ds(k * 2 * pst, 2 * pst)
        src = pl.ds(g * gch, gch)
        push[h, at, lanes] = jnp.concatenate([imap[0, src], imap[1, src]], axis=1).astype(bf16)
        pull[h, at, lanes] = jnp.concatenate([omap[0, src], -omap[1, src]], axis=1).astype(bf16)
    loads_a[10].wait()
    for g in range(groups):
        old_re = state[pl.ds(g, R, stride=groups), :]
        old_im = state[pl.ds(R * groups + g, R, stride=groups), :]
        straight = jnp.concatenate([old_re, old_im], axis=1)
        swapped = jnp.concatenate([old_im, old_re], axis=1)
        moved[:, pl.ds(g * 2 * pst, 2 * pst)] = (
            coef[0, g:g + 1, :] * straight + coef[1, g:g + 1, :] * swapped
        )
    loads_a[6].wait()
    loads_a[7].wait()
    for c in loads_b:
        c.start()
    projected = jnp.dot(xv[...], w_in[...], preferred_element_type=f32).astype(bf16)
    loads_a[8].wait()
    loads_a[9].wait()
    scores = rw[...]
    scores = scores / jnp.sum(scores, axis=0, keepdims=True) * route_scale
    expert = lax.broadcasted_iota(jnp.int32, (experts, R), 0)
    table = jnp.zeros((experts, R), f32)
    for k in range(top_k):
        table += jnp.where(ids[k:k + 1, :] == expert, scores[k:k + 1, :], 0.0)
    for o in range(n_ep):
        wsend[o, pl.ds(0, local_experts), pl.ds(0, R)] = table[
            o * local_experts:(o + 1) * local_experts
        ]
    wrecv[e] = wsend[e]
    responses = []
    for h in range(lumps):
        pushed = jnp.dot(
            projected[:, h * 128:(h + 1) * 128], push[h], preferred_element_type=f32
        )
        fresh = []
        for k in range(lump):
            g = h * lump + k
            lanes = pl.ds(g * 2 * pst, 2 * pst)
            straight = pushed[:, k * 2 * pst:(k + 1) * 2 * pst]
            swapped = pltpu.roll(straight, pst, 1)
            new = moved[:, lanes] + (
                coef[2, g:g + 1, :] * straight + coef[3, g:g + 1, :] * swapped
            )
            moved[:, lanes] = new
            fresh.append(new)
        fresh = jnp.concatenate(fresh, axis=1).astype(bf16)
        responses.append(lax.dot_general(fresh, pull[h], NT, preferred_element_type=f32))
    response = jnp.concatenate(responses, axis=1) + skip_row * projected.astype(f32)
    act[t] = jax.nn.gelu(response).astype(bf16)
    pl.semaphore_wait(barrier, n_ep)
    swap = remote(act.at[t], act.at[t], act_s, act_r, {"tp": 1 - t})
    swap.start()

    @pl.loop(1, n_ep)
    def _(k):
        route((e + k) % n_ep).start()

    loads_a[13].wait()
    logits = jnp.dot(
        act[t], glu[pl.ds(pl.multiple_of(t * chans, chans), chans), :],
        preferred_element_type=f32,
    )
    loads_a[14].wait()
    loads_a[11].wait()
    loads_a[12].wait()
    remote(act.at[1 - t], act.at[1 - t], act_s, act_r, {"tp": 1 - t}).wait_recv()
    logits += jnp.dot(
        act[1 - t], glu[pl.ds(pl.multiple_of((1 - t) * chans, chans), chans), :],
        preferred_element_type=f32,
    )
    every = jnp.concatenate([act[0], act[1]], axis=1)
    glu_out = (every.astype(f32) * jax.nn.sigmoid(logits)).astype(bf16)
    mixed = jnp.dot(glu_out, mix[...], preferred_element_type=f32).astype(bf16)
    values = residual_alpha * xv[...].astype(f32) + mixed.astype(f32)
    values = values - jnp.mean(values, axis=1, keepdims=True)
    variance = jnp.mean(jnp.square(values), axis=1, keepdims=True)
    nrm[...] = (values * lax.rsqrt(variance + norm_eps) * ngain[...] + nshift[...]).astype(bf16)
    rows[t, z, a, b] = nrm[:, mine]

    @pl.loop(1, nz)
    def _(s):
        line_copy(event(s)).start()

    one(z, b).start()
    twoa(z).start()

    def shared():
        for g in range(groups):
            at = g * 2 * pst
            new_state[pl.ds(g, R, stride=groups), :] = moved[:, at:at + pst]
            new_state[pl.ds(R * groups + g, R, stride=groups), :] = moved[
                :, at + pst:at + 2 * pst
            ]
        fetched(sgu, 0)
        fetched(sd, 1)
        gu = jnp.dot(nrm[...], sgu[...], preferred_element_type=f32)
        sh = (jax.nn.silu(gu[:, :hid]) * gu[:, hid:]).astype(bf16)
        sh_own[...] = jnp.dot(sh, sd[:, mine], preferred_element_type=f32)
        sh_oth[...] = jnp.dot(sh, sd[:, peers], preferred_element_type=f32)
        fetched(wgu, 2)
        fetched(wd, 3)
        fetched(din.at[pl.ds(0, dense_hid)], 4)
        fetched(dout, 5)
        fetched(bgate, 6)
        fetched(fnorm, 7)
        gate = bgate[...].astype(f32)
        gate = jnp.concatenate([gate[k:k + 1] for k in range(gate.shape[0])], axis=1)
        din[pl.ds(dense_hid, 1), :] = gate.astype(bf16)

    blocks = [(k // 2, k % 2) for k in range(4)]

    def near_half(s, j):
        mine_x = jnp.concatenate([rows[t, j, aa, bb] for aa, bb in blocks], axis=0)
        for l in range(local_experts):
            gacc[s % 2, l] = jnp.dot(mine_x, wgu[l, mine, :], preferred_element_type=f32)
        dacc[s % 2] = lax.dot_general(mine_x, din[:, mine], NT, preferred_element_type=f32)

    def far_half(s, j):
        d_wait(j)
        if s == 0:
            routes().wait_recv()
        peer_x = jnp.concatenate([rows[1 - t, j, bb, aa] for aa, bb in blocks], axis=0)
        oth_part = None
        for l in range(local_experts):
            w = jnp.concatenate(
                [
                    column(
                        wrecv[
                            j * 4 + (aa * (1 - t) + bb * t) * 2 + bb * (1 - t) + aa * t,
                            l:l + 1, 0:R,
                        ],
                        R,
                    )
                    for aa, bb in blocks
                ],
                axis=0,
            )
            g = gacc[s % 2, l] + jnp.dot(peer_x, wgu[l, peers, :], preferred_element_type=f32)
            h = (jax.nn.silu(g[:, :ffn]) * g[:, ffn:] * w).astype(bf16)
            hbuf[s % 2, l] = h
            o = jnp.dot(h, wd[l, :, peers], preferred_element_type=f32)
            oth_part = o if oth_part is None else oth_part + o
        oth_part = oth_part.astype(bf16).reshape(4, R, half)
        for k, (aa, bb) in enumerate(blocks):
            pbuf[j, bb, aa] = oth_part[k]

        if s == 0:
            pbuf[j, b, a] = (pbuf[j, b, a].astype(f32) + sh_oth[...]).astype(bf16)
        part(j).start()

    def down(s, j):
        peer_x = jnp.concatenate([rows[1 - t, j, bb, aa] for aa, bb in blocks], axis=0)
        d = dacc[s % 2] + lax.dot_general(
            peer_x, din[:, peers], NT, preferred_element_type=f32
        )
        branch = jax.nn.sigmoid(d[:, dense_hid:dense_hid + 1])
        dh = (jax.nn.gelu(d[:, :dense_hid]) * branch).astype(bf16)
        own_part = jnp.dot(dh, dout[...], preferred_element_type=f32)
        for l in range(local_experts):
            own_part += jnp.dot(hbuf[s % 2, l], wd[l, :, mine], preferred_element_type=f32)
        own[j] = own_part.reshape(2, 2, R, half)

    def stage_a(s, j):
        line_wait(j)
        one(j, b).start()

    def stage_t(s, j):
        twoa(j).start()

    def stage_b(s, j):
        one(j, 1 - b).wait_recv()
        twob(j).start()
        da(j).start()

    def stage_c(s, j):
        two_wait(j)
        db(j).start()

    def stage_e(s, j):
        part(j).wait_recv()
        comb[j] = (own[j] + precv[j].astype(f32)).astype(bf16)
        firstx(j).start()

    def stage_y(s, j):
        firsty(j).start()

    def stage_f(s, j):
        firstx(j).wait_recv()
        s2buf[j] = (comb[j, a, 1 - b].astype(f32) + rs1[j, 1 - b].astype(f32)).astype(bf16)
        second(j).start()

    def stage_g(s, j):
        g_wait(j)
        summed = comb[j, a, b].astype(f32) + rs1[j, b].astype(f32) + rs2[j].astype(f32)

        if s == 0:
            acc[...] = summed + sh_own[...] + residual_alpha * nrm[:, mine].astype(f32)
        else:
            t3buf[j] = summed.astype(bf16)
            third(j).start()

    runs = dict(
        A=stage_a, B=stage_b, C=stage_c, P=near_half, Q=far_half, R=down, E=stage_e, F=stage_f,
        G=stage_g, T=stage_t, Y=stage_y,
    )
    extra = [name + str(j) for j in range(4, nz) for name in "ATBCPQREYFG"]
    for item in list(order) + extra:
        if item == "H":
            shared()
        else:
            s = int(item[1:])
            runs[item[0]](s, event(s))

    thirds().wait_recv()

    @pl.loop(1, nz)
    def _(s):
        j = event(s)
        acc[...] += t3recv[j].astype(f32)

    total = acc[...]
    lane = lax.broadcasted_iota(jnp.int32, stat.shape, 1)
    row_sum = jnp.sum(total, axis=1, keepdims=True)
    row_sq = jnp.sum(total * total, axis=1, keepdims=True)
    stat[...] = jnp.where(lane == 0, row_sum, row_sq)
    exchange = remote(stat, statr, stat_s, stat_r, {"tp": 1 - t})
    exchange.start()
    swap.wait_send()

    routes().wait_send()

    each = rows.at[0, :, 0, 0]
    for sem in (one_s, twoa_s, twob_s, fx_s, fy_s, rs2_s):
        sent(each, sem)
    for sem in (da_s, db_s):
        sent(rows.at[0, :, 0], sem)
    sent(pbuf, p_s)
    sent(rows.at[0, lines, 0, 0], line_s)
    thirds().wait_send()
    exchange.wait()
    mean = (row_sum + statr[:, 0:1]) / width
    variance = (row_sq + statr[:, 1:2]) / width - mean * mean
    out[...] = (
        (total - mean) * lax.rsqrt(variance + norm_eps) * fnorm[0:1] + fnorm[1:2]
    ).astype(bf16)


def write_kernel(layer_v, state_v, layer_o, state_o, sems):
    copies = [
        pltpu.make_async_copy(state_v, state_o, sems.at[0]),
        pltpu.make_async_copy(layer_v, layer_o, sems.at[1]),
    ]
    for c in copies:
        c.start()
    for c in copies:
        c.wait()


def body(
    layer_input, ssm_state, w_input, decay_rate, frequency, step_log, input_map, output_map,
    skip_gain, glu_weight, mix_out, norm_gain, norm_shift, route_ids, route_weights,
    gate_expert, up_expert, down_expert, gate_shared, up_shared, down_shared,
    dense_in, dense_out, branch_gate, final_gain, final_shift,
):
    n_ep = lax.axis_size("ep")
    R, width = layer_input.shape
    half = width // 2
    local_experts, _, ffn = gate_expert.shape
    hid = gate_shared.shape[1]
    dense_hid = dense_in.shape[0]
    groups, gch = skip_gain.shape
    pst = decay_rate.shape[1]
    chans = groups * gch
    top_k = route_ids.shape[1]
    nz = n_ep // 4
    lumps = chans // 128
    wide = (128 // gch) * 2 * pst
    dense_pad = -(-(dense_hid + 1) // 128) * 128
    exp_pad = -(-local_experts // 8) * 8
    operands = (
        layer_input,
        ssm_state.reshape(2 * R * groups, pst),
        w_input,
        decay_rate,
        frequency,
        step_log[None, :],
        input_map.transpose(0, 1, 3, 2).reshape(2, chans, pst),
        output_map.reshape(2, chans, pst),
        skip_gain,
        glu_weight,
        mix_out,
        norm_gain[None, :],
        norm_shift[None, :],
        route_ids.T,
        route_weights.T,
        gate_expert, up_expert, down_expert, gate_shared, up_shared, down_shared,
        dense_in, dense_out,
        branch_gate.reshape(width // 128, 128),
        final_gain[None, :],
        final_shift[None, :],
    )
    hbm = pl.BlockSpec(memory_space=pl.ANY)
    vmem = pl.BlockSpec(memory_space=pltpu.VMEM)
    dma = pltpu.SemaphoreType.DMA

    def like(i):
        return pltpu.VMEM(operands[i].shape, operands[i].dtype)

    layer_output, new_state = pl.pallas_call(
        functools.partial(layer_kernel, n_ep, local_experts),
        out_shape=(
            pltpu.VMEM((R, half), bf16),
            pltpu.VMEM((2 * R * groups, pst), f32),
        ),
        in_specs=[hbm] * len(operands),
        out_specs=(vmem, vmem),
        scratch_shapes=[like(i) for i in range(15)]
        + [like(23), pltpu.VMEM((2, half), f32)]
        + [
            pltpu.VMEM((lumps, 128, wide), bf16),
            pltpu.VMEM((lumps, 128, wide), bf16),
            pltpu.VMEM((4, groups, 2 * pst), f32),
            pltpu.VMEM((R, groups * 2 * pst), f32),
            pltpu.VMEM((2, R, chans), bf16),
            pltpu.VMEM((R, width), bf16),
            pltpu.VMEM((n_ep, exp_pad, 128), f32),
            pltpu.VMEM((n_ep, exp_pad, 128), f32),
            pltpu.VMEM((2, nz, 2, 2, R, half), bf16),
            pltpu.VMEM((local_experts, width, 2 * ffn), bf16),
            pltpu.VMEM((local_experts, ffn, width), bf16),
            pltpu.VMEM((width, 2 * hid), bf16),
            pltpu.VMEM((hid, width), bf16),
            pltpu.VMEM((dense_pad, width), bf16),
            pltpu.VMEM((dense_hid, half), bf16),
            pltpu.VMEM((nz, 2, 2, R, half), f32),
            pltpu.VMEM((2, local_experts, 4 * R, 2 * ffn), f32),
            pltpu.VMEM((2, 4 * R, dense_pad), f32),
            pltpu.VMEM((2, local_experts, 4 * R, ffn), bf16),
            pltpu.VMEM((nz, 2, 2, R, half), bf16),
            pltpu.VMEM((nz, 2, 2, R, half), bf16),
            pltpu.VMEM((nz, 2, 2, R, half), bf16),
            pltpu.VMEM((nz, 2, R, half), bf16),
            pltpu.VMEM((nz, R, half), bf16),
            pltpu.VMEM((nz, R, half), bf16),
            pltpu.VMEM((nz, R, half), bf16),
            pltpu.VMEM((nz, R, half), bf16),
            pltpu.VMEM((R, half), f32),
            pltpu.VMEM((R, half), f32),
            pltpu.VMEM((R, half), f32),
            pltpu.VMEM((R, 128), f32),
            pltpu.VMEM((R, 128), f32),
            dma((15,)),
            dma((8,)),
            dma,
            dma,
        ]
        + [dma((nz,))] * 7
        + [dma] * 16,
        compiler_params=pltpu.CompilerParams(
            collective_id=0, has_side_effects=True, vmem_limit_bytes=60 * 1024 * 1024
        ),
    )(*operands)
    layer_output, new_state = pl.pallas_call(
        write_kernel,
        out_shape=(
            jax.ShapeDtypeStruct((R, half), bf16),
            jax.ShapeDtypeStruct((2 * R * groups, pst), f32),
        ),
        in_specs=[vmem, vmem],
        out_specs=(hbm, hbm),
        scratch_shapes=[dma((2,))],
    )(
        pltpu.with_memory_space_constraint(layer_output, pltpu.VMEM),
        pltpu.with_memory_space_constraint(new_state, pltpu.VMEM),
    )
    return (layer_output, new_state.reshape(2, R, groups, pst))


def solution(mesh):
    placed = (
        P(("grp", "ep"), None),
        P(None, ("grp", "ep"), "tp", None),
        P(None, "tp"),
        P("tp", None),
        P("tp", None),
        P("tp"),
        P(None, "tp", None, None),
        P(None, "tp", None, None),
        P("tp", None),
        P(),
        P(),
        P(),
        P(),
        P(("grp", "ep"), None),
        P(("grp", "ep"), None),
        P("ep", None, "tp"),
        P("ep", None, "tp"),
        P("ep", "tp", None),
        P(None, "tp"),
        P(None, "tp"),
        P("tp", None),
        P("ep", None),
        P("ep", "tp"),
        P(),
        P("tp"),
        P("tp"),
    )
    return jax.shard_map(
        body,
        mesh=mesh,
        in_specs=placed,
        out_specs=(P(("grp", "ep"), "tp"), P(None, ("grp", "ep"), "tp", None)),
        check_vma=False,
    )
```

```python
import functools

import jax
import jax.numpy as jnp
from jax import lax
from jax.experimental import pallas as pl
from jax.experimental.pallas import tpu as pltpu
from jax.sharding import PartitionSpec as P

residual_alpha = 1.681792830507429
route_scale = 2.5
norm_eps = 1e-05
MESH = pl.DeviceIdType.MESH
f32 = jnp.float32
bf16 = jnp.bfloat16
NT = (((1,), (1,)), ((), ()))

order = (
    "H", "B0", "A1", "T1", "C0", "P0", "A2", "B1", "T2", "A3", "Q0", "R0", "B2", "T3", "C1",
    "E0", "P1", "B3", "Y0", "Q1", "C2", "R1", "P2", "E1", "Y1", "Q2", "C3", "F0", "P3", "R2",
    "E2", "Y2", "Q3", "F1", "R3", "E3", "Y3", "F2", "G1", "F3", "G2", "G0", "G3",
)


def column(row, size):
    rows = lax.broadcasted_iota(jnp.int32, (size, size), 0)
    lanes = lax.broadcasted_iota(jnp.int32, (size, size), 1)
    return jnp.sum(jnp.where(rows == lanes, row, 0.0), axis=1, keepdims=True)


def layer_kernel(
    n_ep, local_experts,
    x_h, state_h, w_in_h, decay_h, freq_h, step_h, imap_h, omap_h, skip_h, glu_h, mix_h, ngain_h,
    nshift_h, ids_h, rw_h, gate_e, up_e, down_e, gate_s, up_s, down_s, dense_in, dense_out,
    bgate_h, fgain_h, fshift_h,
    out, new_state,
    xv, state, w_in, decay, freq, step, imap, omap, skip, glu, mix, ngain, nshift, ids, rw,
    bgate, fnorm, push, pull, coef, moved, kept, act, nrm, wsend, wrecv,
    rows, wgu, wd, sgu, sd, din, dout,
    own, gacc, dacc, hbuf, pbuf, precv, comb, rs1, s2buf, rs2, t3buf, t3recv, acc, sh_own, sh_oth, stat, statr,
    asem, wsem,
    route_s, route_r,
    line_r, one_r, two_r, d_r, p_r, fx_r, g_r,
    t3_r, line_s, one_s, db_s, p_s, t3_s,
    act_s, act_r, stat_s, stat_r,
):
    nz = n_ep // 4
    R, width = xv.shape
    half = width // 2
    hid = gate_s.shape[1]
    ffn = gate_e.shape[2]
    dense_hid = dense_in.shape[0]
    chans = w_in.shape[1]
    groups, pst = decay.shape
    gch = chans // groups
    top_k = ids.shape[0]
    experts = n_ep * local_experts
    t = lax.axis_index("tp")
    e = lax.axis_index("ep")
    z = e // 4
    y = (e % 4) // 2
    x = e % 2
    a = y * (1 - t) + x * t
    b = x * (1 - t) + y * t
    ep_b = z * 4 + y * 2 + x + (1 - 2 * x) * (1 - t) + 2 * (1 - 2 * y) * t
    ep_a = z * 4 + y * 2 + x + (1 - 2 * x) * t + 2 * (1 - 2 * y) * (1 - t)

    def line_ep(other):
        return other * 4 + y * 2 + x

    mine = pl.ds(pl.multiple_of(t * half, half), half)
    peers = pl.ds(pl.multiple_of((1 - t) * half, half), half)

    first_loads = [
        (step_h, step), (decay_h, decay), (freq_h, freq), (imap_h, imap), (omap_h, omap),
        (skip_h, skip), (x_h, xv), (w_in_h, w_in), (ids_h, ids), (rw_h, rw), (state_h, state),
        (ngain_h, ngain), (nshift_h, nshift), (glu_h, glu), (mix_h, mix),
    ]
    loads_a = [
        pltpu.make_async_copy(s, d, asem.at[(i > 10) + (i == 13)])
        for i, (s, d) in enumerate(first_loads)
    ]
    fetch = [
        (gate_s, sgu.at[:, pl.ds(0, hid)]),
        (up_s, sgu.at[:, pl.ds(hid, hid)]),
        (down_s, sd),
    ]
    for l in range(local_experts):
        fetch += [
            (gate_e.at[l], wgu.at[l, :, pl.ds(0, ffn)]),
            (up_e.at[l], wgu.at[l, :, pl.ds(ffn, ffn)]),
        ]
    fetch += [
        (down_e, wd),
        (dense_in, din.at[pl.ds(0, dense_hid)]),
        (dense_out, dout),
        (bgate_h, bgate),
        (fgain_h, fnorm.at[0:1]),
        (fshift_h, fnorm.at[1:2]),
    ]
    loads_b = [pltpu.make_async_copy(src, dst, wsem) for src, dst in fetch]

    for i in (7, 6, 5, 4, 3, 2, 1, 0, 10, 8, 9, 11, 12):
        loads_a[i].start()

    barrier = pltpu.get_barrier_semaphore()
    pl.semaphore_signal(barrier, inc=1, device_id={"tp": 1 - t}, device_id_type=MESH)

    @pl.loop(1, n_ep)
    def _(k):
        pl.semaphore_signal(
            barrier, inc=1, device_id={"ep": (e + k) % n_ep}, device_id_type=MESH
        )

    def remote(src, dst, ss, rs, where):
        return pltpu.make_async_remote_copy(
            src_ref=src, dst_ref=dst, send_sem=ss, recv_sem=rs,
            device_id=where, device_id_type=MESH,
        )

    def event(s):
        if isinstance(s, int) and s == 0:
            return z
        return jnp.where(s - 1 >= z, s, s - 1)

    def route(other):
        return remote(wsend.at[other], wrecv.at[e], route_s, route_r, {"ep": other})

    def routes():
        most = pl.ds(0, n_ep - 1)
        return remote(wsend.at[most], wrecv.at[most], route_s, route_r, {"ep": (e + 1) % n_ep})

    def line_copy(other):
        return remote(rows.at[t, z, a, b], rows.at[t, z, a, b], line_s, line_r.at[z],
                      {"ep": line_ep(other)})

    def line_wait(j):
        remote(rows.at[t, j, a, b], rows.at[t, j, a, b], line_s, line_r.at[j],
               {"ep": ep_a}).wait_recv()

    def one(j, at):
        return remote(rows.at[t, j, a, at], rows.at[t, j, a, at], one_s, one_r.at[j],
                      {"ep": ep_b})

    def twoa(j):
        return remote(rows.at[t, j, a, b], rows.at[t, j, a, b], one_s, two_r.at[j],
                      {"ep": ep_a})

    def twob(j):
        return remote(rows.at[t, j, a, 1 - b], rows.at[t, j, a, 1 - b], one_s, two_r.at[j],
                      {"ep": ep_a})

    def two_wait(j):
        remote(rows.at[t, j, 1 - a], rows.at[t, j, 1 - a], one_s, two_r.at[j],
               {"ep": ep_a}).wait_recv()

    def da(j):
        return remote(rows.at[t, j, a], rows.at[t, j, a], one_s, d_r.at[j], {"tp": 1 - t})

    def db(j):
        return remote(rows.at[t, j, 1 - a], rows.at[t, j, 1 - a], db_s, d_r.at[j],
                      {"tp": 1 - t})

    def d_wait(j):
        remote(rows.at[1 - t, j], rows.at[1 - t, j], one_s, d_r.at[j], {"tp": 1 - t}).wait_recv()

    def part(j):
        return remote(pbuf.at[j], precv.at[j], p_s, p_r.at[j], {"tp": 1 - t})

    def firstx(j):
        return remote(comb.at[j, 1 - a, 1 - b], rs1.at[j, 1 - b], one_s, fx_r.at[j],
                      {"ep": ep_a})

    def firsty(j):
        return remote(comb.at[j, 1 - a, b], rs1.at[j, b], one_s, g_r.at[j], {"ep": ep_a})

    def second(j):
        return remote(s2buf.at[j], rs2.at[j], one_s, g_r.at[j], {"ep": ep_b})

    def g_wait(j):
        remote(rs1.at[j], rs1.at[j], one_s, g_r.at[j], {"ep": ep_b}).wait_recv()

    def third(j):
        return remote(t3buf.at[j], t3recv.at[z], t3_s, t3_r, {"ep": line_ep(j)})

    lines = pl.ds(0, nz - 1)

    def thirds():
        return remote(t3buf.at[lines], t3recv.at[lines], t3_s, t3_r, {"ep": ep_a})

    def sent(ref, sem):
        remote(ref, ref, sem, t3_r, {"ep": ep_a}).wait_send()

    push[...] = jnp.zeros(push.shape, bf16)
    pull[...] = jnp.zeros(pull.shape, bf16)
    wsend[...] = jnp.zeros(wsend.shape, f32)
    din[pl.ds(dense_hid, din.shape[0] - dense_hid), :] = jnp.zeros(
        (din.shape[0] - dense_hid, width), bf16
    )
    for c in loads_a[13:]:
        c.start()
    for c in loads_a[:11]:
        c.wait()
    for c in loads_b:
        c.start()
    size = column(jnp.exp(step[...]), groups)
    rate = decay[...]
    turn = freq[...]
    magnitude = jnp.exp(-rate * size)
    rotation = turn * size
    decay_re = magnitude * jnp.cos(rotation)
    decay_im = magnitude * jnp.sin(rotation)
    denominator = rate * rate + turn * turn
    factor_re = (decay_im * turn - (decay_re - 1.0) * rate) / denominator
    factor_im = (-decay_im * rate - (decay_re - 1.0) * turn) / denominator
    coef[0] = jnp.concatenate([decay_re, decay_re], axis=1)
    coef[1] = jnp.concatenate([-decay_im, decay_im], axis=1)
    coef[2] = jnp.concatenate([factor_re, factor_re], axis=1)
    coef[3] = jnp.concatenate([-factor_im, factor_im], axis=1)
    spread = (
        lax.broadcasted_iota(jnp.int32, (gch, chans), 1) % gch
        == lax.broadcasted_iota(jnp.int32, (gch, chans), 0)
    ).astype(f32)
    tiled = jnp.dot(
        skip[...], spread, precision=lax.Precision.HIGHEST, preferred_element_type=f32
    )
    picked = (
        lax.broadcasted_iota(jnp.int32, (groups, chans), 1) // gch
        == lax.broadcasted_iota(jnp.int32, (groups, chans), 0)
    )
    skip_row = jnp.sum(jnp.where(picked, tiled, 0.0), axis=0, keepdims=True)
    lump = 128 // gch
    lumps = chans // 128
    for g in range(groups):
        h, k = g // lump, g % lump
        at = pl.ds(k * gch, gch)
        lanes = pl.ds(k * 2 * pst, 2 * pst)
        src = pl.ds(g * gch, gch)
        push[h, at, lanes] = jnp.concatenate([imap[0, src], imap[1, src]], axis=1).astype(bf16)
        pull[h, at, lanes] = jnp.concatenate([omap[0, src], -omap[1, src]], axis=1).astype(bf16)
    for g in range(groups):
        old_re = state[pl.ds(g, R, stride=groups), :]
        old_im = state[pl.ds(R * groups + g, R, stride=groups), :]
        straight = jnp.concatenate([old_re, old_im], axis=1)
        swapped = jnp.concatenate([old_im, old_re], axis=1)
        moved[:, pl.ds(g * 2 * pst, 2 * pst)] = (
            coef[0, g:g + 1, :] * straight + coef[1, g:g + 1, :] * swapped
        )
    projected = jnp.dot(xv[...], w_in[...], preferred_element_type=f32).astype(bf16)
    scores = rw[...]
    scores = scores / jnp.sum(scores, axis=0, keepdims=True) * route_scale
    expert = lax.broadcasted_iota(jnp.int32, (experts, R), 0)
    table = jnp.zeros((experts, R), f32)
    for k in range(top_k):
        table += jnp.where(ids[k:k + 1, :] == expert, scores[k:k + 1, :], 0.0)
    for o in range(n_ep):
        wsend[o, pl.ds(0, local_experts), pl.ds(0, R)] = table[
            o * local_experts:(o + 1) * local_experts
        ]
    wrecv[e] = wsend[e]
    responses = []
    for h in range(lumps):
        pushed = jnp.dot(
            projected[:, h * 128:(h + 1) * 128], push[h], preferred_element_type=f32
        )
        fresh = []
        for k in range(lump):
            g = h * lump + k
            lanes = pl.ds(g * 2 * pst, 2 * pst)
            straight = pushed[:, k * 2 * pst:(k + 1) * 2 * pst]
            swapped = pltpu.roll(straight, pst, 1)
            new = moved[:, lanes] + (
                coef[2, g:g + 1, :] * straight + coef[3, g:g + 1, :] * swapped
            )
            kept[:, lanes] = new
            fresh.append(new)
        fresh = jnp.concatenate(fresh, axis=1).astype(bf16)
        responses.append(lax.dot_general(fresh, pull[h], NT, preferred_element_type=f32))
    response = jnp.concatenate(responses, axis=1) + skip_row * projected.astype(f32)
    act[t] = jax.nn.gelu(response).astype(bf16)
    pl.semaphore_wait(barrier, n_ep)
    swap = remote(act.at[t], act.at[t], act_s, act_r, {"tp": 1 - t})
    swap.start()

    @pl.loop(1, n_ep)
    def _(k):
        route((e + k) % n_ep).start()

    loads_a[13].wait()
    logits = jnp.dot(
        act[t], glu[pl.ds(pl.multiple_of(t * chans, chans), chans), :],
        preferred_element_type=f32,
    )
    loads_a[14].wait()
    loads_a[11].wait()
    loads_a[12].wait()
    remote(act.at[1 - t], act.at[1 - t], act_s, act_r, {"tp": 1 - t}).wait_recv()
    logits += jnp.dot(
        act[1 - t], glu[pl.ds(pl.multiple_of((1 - t) * chans, chans), chans), :],
        preferred_element_type=f32,
    )
    every = jnp.concatenate([act[0], act[1]], axis=1)
    glu_out = (every.astype(f32) * jax.nn.sigmoid(logits)).astype(bf16)
    mixed = jnp.dot(glu_out, mix[...], preferred_element_type=f32).astype(bf16)
    values = residual_alpha * xv[...].astype(f32) + mixed.astype(f32)
    values = values - jnp.mean(values, axis=1, keepdims=True)
    variance = jnp.mean(jnp.square(values), axis=1, keepdims=True)
    nrm[...] = (values * lax.rsqrt(variance + norm_eps) * ngain[...] + nshift[...]).astype(bf16)
    rows[t, z, a, b] = nrm[:, mine]

    @pl.loop(1, nz)
    def _(s):
        line_copy(event(s)).start()

    one(z, b).start()
    twoa(z).start()

    def shared():
        for g in range(groups):
            at = g * 2 * pst
            new_state[pl.ds(g, R, stride=groups), :] = kept[:, at:at + pst]
            new_state[pl.ds(R * groups + g, R, stride=groups), :] = kept[
                :, at + pst:at + 2 * pst
            ]
        for c in loads_b:
            c.wait()
        gu = jnp.dot(nrm[...], sgu[...], preferred_element_type=f32)
        sh = (jax.nn.silu(gu[:, :hid]) * gu[:, hid:]).astype(bf16)
        sh_own[...] = jnp.dot(sh, sd[:, mine], preferred_element_type=f32)
        sh_oth[...] = jnp.dot(sh, sd[:, peers], preferred_element_type=f32)
        gate = bgate[...].astype(f32)
        gate = jnp.concatenate([gate[k:k + 1] for k in range(gate.shape[0])], axis=1)
        din[pl.ds(dense_hid, 1), :] = gate.astype(bf16)

    blocks = [(k // 2, k % 2) for k in range(4)]

    def near_half(s, j):
        mine_x = jnp.concatenate([rows[t, j, aa, bb] for aa, bb in blocks], axis=0)
        for l in range(local_experts):
            gacc[s % 2, l] = jnp.dot(mine_x, wgu[l, mine, :], preferred_element_type=f32)
        dacc[s % 2] = lax.dot_general(mine_x, din[:, mine], NT, preferred_element_type=f32)

    def far_half(s, j):
        d_wait(j)
        if s == 0:
            routes().wait_recv()
        peer_x = jnp.concatenate([rows[1 - t, j, bb, aa] for aa, bb in blocks], axis=0)
        oth_part = None
        for l in range(local_experts):
            w = jnp.concatenate(
                [
                    column(
                        wrecv[
                            j * 4 + (aa * (1 - t) + bb * t) * 2 + bb * (1 - t) + aa * t,
                            l:l + 1, 0:R,
                        ],
                        R,
                    )
                    for aa, bb in blocks
                ],
                axis=0,
            )
            g = gacc[s % 2, l] + jnp.dot(peer_x, wgu[l, peers, :], preferred_element_type=f32)
            h = (jax.nn.silu(g[:, :ffn]) * g[:, ffn:] * w).astype(bf16)
            hbuf[s % 2, l] = h
            o = jnp.dot(h, wd[l, :, peers], preferred_element_type=f32)
            oth_part = o if oth_part is None else oth_part + o
        oth_part = oth_part.astype(bf16).reshape(4, R, half)
        for k, (aa, bb) in enumerate(blocks):
            pbuf[j, bb, aa] = oth_part[k]

        if s == 0:
            pbuf[j, b, a] = (pbuf[j, b, a].astype(f32) + sh_oth[...]).astype(bf16)
        part(j).start()

    def down(s, j):
        peer_x = jnp.concatenate([rows[1 - t, j, bb, aa] for aa, bb in blocks], axis=0)
        d = dacc[s % 2] + lax.dot_general(
            peer_x, din[:, peers], NT, preferred_element_type=f32
        )
        branch = jax.nn.sigmoid(d[:, dense_hid:dense_hid + 1])
        dh = (jax.nn.gelu(d[:, :dense_hid]) * branch).astype(bf16)
        own_part = jnp.dot(dh, dout[...], preferred_element_type=f32)
        for l in range(local_experts):
            own_part += jnp.dot(hbuf[s % 2, l], wd[l, :, mine], preferred_element_type=f32)
        own[j] = own_part.reshape(2, 2, R, half)

    def stage_a(s, j):
        line_wait(j)
        one(j, b).start()

    def stage_t(s, j):
        twoa(j).start()

    def stage_b(s, j):
        one(j, 1 - b).wait_recv()
        twob(j).start()
        da(j).start()

    def stage_c(s, j):
        two_wait(j)
        db(j).start()

    def stage_e(s, j):
        part(j).wait_recv()
        comb[j] = (own[j] + precv[j].astype(f32)).astype(bf16)
        firstx(j).start()

    def stage_y(s, j):
        firsty(j).start()

    def stage_f(s, j):
        firstx(j).wait_recv()
        s2buf[j] = (comb[j, a, 1 - b].astype(f32) + rs1[j, 1 - b].astype(f32)).astype(bf16)
        second(j).start()

    def stage_g(s, j):
        g_wait(j)
        summed = comb[j, a, b].astype(f32) + rs1[j, b].astype(f32) + rs2[j].astype(f32)

        if s == 0:
            acc[...] = summed + sh_own[...] + residual_alpha * nrm[:, mine].astype(f32)
        else:
            t3buf[j] = summed.astype(bf16)
            third(j).start()

    runs = dict(
        A=stage_a, B=stage_b, C=stage_c, P=near_half, Q=far_half, R=down, E=stage_e, F=stage_f,
        G=stage_g, T=stage_t, Y=stage_y,
    )
    extra = [name + str(j) for j in range(4, nz) for name in "ATBCPQREYFG"]
    for item in list(order) + extra:
        if item == "H":
            shared()
        else:
            s = int(item[1:])
            runs[item[0]](s, event(s))

    thirds().wait_recv()

    @pl.loop(1, nz)
    def _(s):
        j = event(s)
        acc[...] += t3recv[j].astype(f32)

    total = acc[...]
    lane = lax.broadcasted_iota(jnp.int32, stat.shape, 1)
    row_sum = jnp.sum(total, axis=1, keepdims=True)
    row_sq = jnp.sum(total * total, axis=1, keepdims=True)
    stat[...] = jnp.where(lane == 0, row_sum, row_sq)
    exchange = remote(stat, statr, stat_s, stat_r, {"tp": 1 - t})
    exchange.start()
    swap.wait_send()

    routes().wait_send()

    sent(rows, one_s)
    sent(rows.at[0, :, 0], db_s)
    sent(pbuf, p_s)
    sent(rows.at[0, lines, 0, 0], line_s)
    thirds().wait_send()
    exchange.wait()
    mean = (row_sum + statr[:, 0:1]) / width
    variance = (row_sq + statr[:, 1:2]) / width - mean * mean
    out[...] = (
        (total - mean) * lax.rsqrt(variance + norm_eps) * fnorm[0:1] + fnorm[1:2]
    ).astype(bf16)


def write_kernel(layer_v, state_v, layer_o, state_o, sems):
    copies = [
        pltpu.make_async_copy(state_v, state_o, sems.at[0]),
        pltpu.make_async_copy(layer_v, layer_o, sems.at[1]),
    ]
    for c in copies:
        c.start()
    for c in copies:
        c.wait()


def body(
    layer_input, ssm_state, w_input, decay_rate, frequency, step_log, input_map, output_map,
    skip_gain, glu_weight, mix_out, norm_gain, norm_shift, route_ids, route_weights,
    gate_expert, up_expert, down_expert, gate_shared, up_shared, down_shared,
    dense_in, dense_out, branch_gate, final_gain, final_shift,
):
    n_ep = lax.axis_size("ep")
    R, width = layer_input.shape
    half = width // 2
    local_experts, _, ffn = gate_expert.shape
    hid = gate_shared.shape[1]
    dense_hid = dense_in.shape[0]
    groups, gch = skip_gain.shape
    pst = decay_rate.shape[1]
    chans = groups * gch
    top_k = route_ids.shape[1]
    nz = n_ep // 4
    lumps = chans // 128
    wide = (128 // gch) * 2 * pst
    dense_pad = -(-(dense_hid + 1) // 128) * 128
    exp_pad = -(-local_experts // 8) * 8
    operands = (
        layer_input,
        ssm_state.reshape(2 * R * groups, pst),
        w_input,
        decay_rate,
        frequency,
        step_log[None, :],
        input_map.transpose(0, 1, 3, 2).reshape(2, chans, pst),
        output_map.reshape(2, chans, pst),
        skip_gain,
        glu_weight,
        mix_out,
        norm_gain[None, :],
        norm_shift[None, :],
        route_ids.T,
        route_weights.T,
        gate_expert, up_expert, down_expert, gate_shared, up_shared, down_shared,
        dense_in, dense_out,
        branch_gate.reshape(width // 128, 128),
        final_gain[None, :],
        final_shift[None, :],
    )
    hbm = pl.BlockSpec(memory_space=pl.ANY)
    vmem = pl.BlockSpec(memory_space=pltpu.VMEM)
    dma = pltpu.SemaphoreType.DMA

    def like(i):
        return pltpu.VMEM(operands[i].shape, operands[i].dtype)

    layer_output, new_state = pl.pallas_call(
        functools.partial(layer_kernel, n_ep, local_experts),
        out_shape=(
            pltpu.VMEM((R, half), bf16),
            pltpu.VMEM((2 * R * groups, pst), f32),
        ),
        in_specs=[hbm] * len(operands),
        out_specs=(vmem, vmem),
        scratch_shapes=[like(i) for i in range(15)]
        + [like(23), pltpu.VMEM((2, half), f32)]
        + [
            pltpu.VMEM((lumps, 128, wide), bf16),
            pltpu.VMEM((lumps, 128, wide), bf16),
            pltpu.VMEM((4, groups, 2 * pst), f32),
            pltpu.VMEM((R, groups * 2 * pst), f32),
            pltpu.VMEM((R, groups * 2 * pst), f32),
            pltpu.VMEM((2, R, chans), bf16),
            pltpu.VMEM((R, width), bf16),
            pltpu.VMEM((n_ep, exp_pad, 128), f32),
            pltpu.VMEM((n_ep, exp_pad, 128), f32),
            pltpu.VMEM((2, nz, 2, 2, R, half), bf16),
            pltpu.VMEM((local_experts, width, 2 * ffn), bf16),
            pltpu.VMEM((local_experts, ffn, width), bf16),
            pltpu.VMEM((width, 2 * hid), bf16),
            pltpu.VMEM((hid, width), bf16),
            pltpu.VMEM((dense_pad, width), bf16),
            pltpu.VMEM((dense_hid, half), bf16),
            pltpu.VMEM((nz, 2, 2, R, half), f32),
            pltpu.VMEM((2, local_experts, 4 * R, 2 * ffn), f32),
            pltpu.VMEM((2, 4 * R, dense_pad), f32),
            pltpu.VMEM((2, local_experts, 4 * R, ffn), bf16),
            pltpu.VMEM((nz, 2, 2, R, half), bf16),
            pltpu.VMEM((nz, 2, 2, R, half), bf16),
            pltpu.VMEM((nz, 2, 2, R, half), bf16),
            pltpu.VMEM((nz, 2, R, half), bf16),
            pltpu.VMEM((nz, R, half), bf16),
            pltpu.VMEM((nz, R, half), bf16),
            pltpu.VMEM((nz, R, half), bf16),
            pltpu.VMEM((nz, R, half), bf16),
            pltpu.VMEM((R, half), f32),
            pltpu.VMEM((R, half), f32),
            pltpu.VMEM((R, half), f32),
            pltpu.VMEM((R, 128), f32),
            pltpu.VMEM((R, 128), f32),
            dma((3,)),
            dma,
            dma,
            dma,
        ]
        + [dma((nz,))] * 7
        + [dma] * 10,
        compiler_params=pltpu.CompilerParams(
            collective_id=0, has_side_effects=True, vmem_limit_bytes=60 * 1024 * 1024
        ),
    )(*operands)
    layer_output, new_state = pl.pallas_call(
        write_kernel,
        out_shape=(
            jax.ShapeDtypeStruct((R, half), bf16),
            jax.ShapeDtypeStruct((2 * R * groups, pst), f32),
        ),
        in_specs=[vmem, vmem],
        out_specs=(hbm, hbm),
        scratch_shapes=[dma((2,))],
    )(
        pltpu.with_memory_space_constraint(layer_output, pltpu.VMEM),
        pltpu.with_memory_space_constraint(new_state, pltpu.VMEM),
    )
    return (layer_output, new_state.reshape(2, R, groups, pst))


def solution(mesh):
    placed = (
        P(("grp", "ep"), None),
        P(None, ("grp", "ep"), "tp", None),
        P(None, "tp"),
        P("tp", None),
        P("tp", None),
        P("tp"),
        P(None, "tp", None, None),
        P(None, "tp", None, None),
        P("tp", None),
        P(),
        P(),
        P(),
        P(),
        P(("grp", "ep"), None),
        P(("grp", "ep"), None),
        P("ep", None, "tp"),
        P("ep", None, "tp"),
        P("ep", "tp", None),
        P(None, "tp"),
        P(None, "tp"),
        P("tp", None),
        P("ep", None),
        P("ep", "tp"),
        P(),
        P("tp"),
        P("tp"),
    )
    return jax.shard_map(
        body,
        mesh=mesh,
        in_specs=placed,
        out_specs=(P(("grp", "ep"), "tp"), P(None, ("grp", "ep"), "tp", None)),
        check_vma=False,
    )
```

```python
import functools

import jax
import jax.numpy as jnp
from jax import lax
from jax.experimental import pallas as pl
from jax.experimental.pallas import tpu as pltpu
from jax.sharding import PartitionSpec as P

residual_alpha = 1.681792830507429
route_scale = 2.5
norm_eps = 1e-05
MESH = pl.DeviceIdType.MESH
f32 = jnp.float32
bf16 = jnp.bfloat16
NT = (((1,), (1,)), ((), ()))

order = (
    "H", "B0", "A1", "T1", "C0", "P0", "A2", "B1", "T2", "A3", "Q0", "R0", "B2", "T3", "C1",
    "E0", "P1", "B3", "Y0", "Q1", "C2", "R1", "P2", "E1", "Y1", "Q2", "C3", "F0", "P3", "R2",
    "E2", "Y2", "Q3", "F1", "R3", "E3", "Y3", "F2", "G1", "F3", "G2", "G0", "G3",
)


def column(row, size):
    rows = lax.broadcasted_iota(jnp.int32, (size, size), 0)
    lanes = lax.broadcasted_iota(jnp.int32, (size, size), 1)
    return jnp.sum(jnp.where(rows == lanes, row, 0.0), axis=1, keepdims=True)


def layer_kernel(
    n_ep, local_experts,
    x_h, state_h, w_in_h, decay_h, freq_h, step_h, imap_h, omap_h, skip_h, glu_h, mix_h, ngain_h,
    nshift_h, ids_h, rw_h, gate_e, up_e, down_e, gate_s, up_s, down_s, dense_in, dense_out,
    bgate_h, fgain_h, fshift_h,
    out, new_state,
    xv, state, w_in, decay, freq, step, imap, omap, skip, glu, mix, ngain, nshift, ids, rw,
    bgate, fnorm, push, pull, coef, moved, kept, act, nrm, wsend, wrecv,
    rows, wgu, wd, sgu, sd, din, dout,
    own, gacc, dacc, hbuf, pbuf, precv, comb, rs1, s2buf, rs2, t3buf, t3recv, acc, sh_own, sh_oth, stat, statr,
    asem, wsem,
    route_s, route_r,
    line_r, one_r, two_r, d_r, p_r, fx_r, g_r,
    t3_r, line_s, one_s, db_s, p_s, t3_s,
    act_s, act_r, stat_s, stat_r,
):
    nz = n_ep // 4
    R, width = xv.shape
    half = width // 2
    hid = gate_s.shape[1]
    ffn = gate_e.shape[2]
    dense_hid = dense_in.shape[0]
    chans = w_in.shape[1]
    groups, pst = decay.shape
    gch = chans // groups
    top_k = ids.shape[0]
    experts = n_ep * local_experts
    t = lax.axis_index("tp")
    e = lax.axis_index("ep")
    z = e // 4
    y = (e % 4) // 2
    x = e % 2
    a = y * (1 - t) + x * t
    b = x * (1 - t) + y * t
    ep_b = z * 4 + y * 2 + x + (1 - 2 * x) * (1 - t) + 2 * (1 - 2 * y) * t
    ep_a = z * 4 + y * 2 + x + (1 - 2 * x) * t + 2 * (1 - 2 * y) * (1 - t)

    def line_ep(other):
        return other * 4 + y * 2 + x

    mine = pl.ds(pl.multiple_of(t * half, half), half)
    peers = pl.ds(pl.multiple_of((1 - t) * half, half), half)

    first_loads = [
        (step_h, step), (decay_h, decay), (freq_h, freq), (imap_h, imap), (omap_h, omap),
        (skip_h, skip), (x_h, xv), (w_in_h, w_in), (ids_h, ids), (rw_h, rw), (state_h, state),
        (ngain_h, ngain), (nshift_h, nshift), (glu_h, glu), (mix_h, mix),
    ]
    loads_a = [
        pltpu.make_async_copy(s, d, asem.at[(i > 10) + (i == 13)])
        for i, (s, d) in enumerate(first_loads)
    ]
    fetch = [
        (gate_s, sgu.at[:, pl.ds(0, hid)]),
        (up_s, sgu.at[:, pl.ds(hid, hid)]),
        (down_s, sd),
    ]
    for l in range(local_experts):
        fetch += [
            (gate_e.at[l], wgu.at[l, :, pl.ds(0, ffn)]),
            (up_e.at[l], wgu.at[l, :, pl.ds(ffn, ffn)]),
        ]
    fetch += [
        (down_e, wd),
        (dense_in, din.at[pl.ds(0, dense_hid)]),
        (dense_out, dout),
        (bgate_h, bgate),
        (fgain_h, fnorm.at[0:1]),
        (fshift_h, fnorm.at[1:2]),
    ]
    loads_b = [pltpu.make_async_copy(src, dst, wsem) for src, dst in fetch]

    for i in (7, 6, 5, 4, 3, 2, 1, 0, 10, 8, 9, 11, 12):
        loads_a[i].start()

    barrier = pltpu.get_barrier_semaphore()
    pl.semaphore_signal(barrier, inc=1, device_id={"tp": 1 - t}, device_id_type=MESH)

    @pl.loop(1, n_ep)
    def _(k):
        pl.semaphore_signal(
            barrier, inc=1, device_id={"ep": (e + k) % n_ep}, device_id_type=MESH
        )

    def remote(src, dst, ss, rs, where):
        return pltpu.make_async_remote_copy(
            src_ref=src, dst_ref=dst, send_sem=ss, recv_sem=rs,
            device_id=where, device_id_type=MESH,
        )

    def event(s):
        if isinstance(s, int) and s == 0:
            return z
        return jnp.where(s - 1 >= z, s, s - 1)

    def route(other):
        return remote(wsend.at[other], wrecv.at[e], route_s, route_r, {"ep": other})

    def routes():
        most = pl.ds(0, n_ep - 1)
        return remote(wsend.at[most], wrecv.at[most], route_s, route_r, {"ep": (e + 1) % n_ep})

    def line_copy(other):
        return remote(rows.at[t, z, a, b], rows.at[t, z, a, b], line_s, line_r.at[z],
                      {"ep": line_ep(other)})

    def line_wait(j):
        remote(rows.at[t, j, a, b], rows.at[t, j, a, b], line_s, line_r.at[j],
               {"ep": ep_a}).wait_recv()

    def one(j, at):
        return remote(rows.at[t, j, a, at], rows.at[t, j, a, at], one_s, one_r.at[j],
                      {"ep": ep_b})

    def twoa(j):
        return remote(rows.at[t, j, a, b], rows.at[t, j, a, b], one_s, two_r.at[j],
                      {"ep": ep_a})

    def twob(j):
        return remote(rows.at[t, j, a, 1 - b], rows.at[t, j, a, 1 - b], one_s, two_r.at[j],
                      {"ep": ep_a})

    def two_wait(j):
        remote(rows.at[t, j, 1 - a], rows.at[t, j, 1 - a], one_s, two_r.at[j],
               {"ep": ep_a}).wait_recv()

    def da(j):
        return remote(rows.at[t, j, a], rows.at[t, j, a], one_s, d_r.at[j], {"tp": 1 - t})

    def db(j):
        return remote(rows.at[t, j, 1 - a], rows.at[t, j, 1 - a], db_s, d_r.at[j],
                      {"tp": 1 - t})

    def d_wait(j):
        remote(rows.at[1 - t, j], rows.at[1 - t, j], one_s, d_r.at[j], {"tp": 1 - t}).wait_recv()

    def part(j):
        return remote(pbuf.at[j], precv.at[j], p_s, p_r.at[j], {"tp": 1 - t})

    def firstx(j):
        return remote(comb.at[j, 1 - a, 1 - b], rs1.at[j, 1 - b], one_s, fx_r.at[j],
                      {"ep": ep_a})

    def firsty(j):
        return remote(comb.at[j, 1 - a, b], rs1.at[j, b], one_s, g_r.at[j], {"ep": ep_a})

    def second(j):
        return remote(s2buf.at[j], rs2.at[j], one_s, g_r.at[j], {"ep": ep_b})

    def g_wait(j):
        remote(rs1.at[j], rs1.at[j], one_s, g_r.at[j], {"ep": ep_b}).wait_recv()

    def third(j):
        return remote(t3buf.at[j], t3recv.at[z], t3_s, t3_r, {"ep": line_ep(j)})

    lines = pl.ds(0, nz - 1)

    def thirds():
        return remote(t3buf.at[lines], t3recv.at[lines], t3_s, t3_r, {"ep": ep_a})

    def sent(ref, sem):
        remote(ref, ref, sem, t3_r, {"ep": ep_a}).wait_send()

    push[...] = jnp.zeros(push.shape, bf16)
    pull[...] = jnp.zeros(pull.shape, bf16)
    wsend[...] = jnp.zeros(wsend.shape, f32)
    din[pl.ds(dense_hid, din.shape[0] - dense_hid), :] = jnp.zeros(
        (din.shape[0] - dense_hid, width), bf16
    )
    for c in loads_a[13:]:
        c.start()
    for c in loads_a[:11]:
        c.wait()
    for c in loads_b:
        c.start()
    size = column(jnp.exp(step[...]), groups)
    rate = decay[...]
    turn = freq[...]
    magnitude = jnp.exp(-rate * size)
    rotation = turn * size
    decay_re = magnitude * jnp.cos(rotation)
    decay_im = magnitude * jnp.sin(rotation)
    denominator = rate * rate + turn * turn
    factor_re = (decay_im * turn - (decay_re - 1.0) * rate) / denominator
    factor_im = (-decay_im * rate - (decay_re - 1.0) * turn) / denominator
    coef[0] = jnp.concatenate([decay_re, decay_re], axis=1)
    coef[1] = jnp.concatenate([-decay_im, decay_im], axis=1)
    coef[2] = jnp.concatenate([factor_re, factor_re], axis=1)
    coef[3] = jnp.concatenate([-factor_im, factor_im], axis=1)
    spread = (
        lax.broadcasted_iota(jnp.int32, (gch, chans), 1) % gch
        == lax.broadcasted_iota(jnp.int32, (gch, chans), 0)
    ).astype(f32)
    tiled = jnp.dot(
        skip[...], spread, precision=lax.Precision.HIGHEST, preferred_element_type=f32
    )
    picked = (
        lax.broadcasted_iota(jnp.int32, (groups, chans), 1) // gch
        == lax.broadcasted_iota(jnp.int32, (groups, chans), 0)
    )
    skip_row = jnp.sum(jnp.where(picked, tiled, 0.0), axis=0, keepdims=True)
    lump = 128 // gch
    lumps = chans // 128
    for g in range(groups):
        h, k = g // lump, g % lump
        at = pl.ds(k * gch, gch)
        lanes = pl.ds(k * 2 * pst, 2 * pst)
        src = pl.ds(g * gch, gch)
        push[h, at, lanes] = jnp.concatenate([imap[0, src], imap[1, src]], axis=1).astype(bf16)
        pull[h, at, lanes] = jnp.concatenate([omap[0, src], -omap[1, src]], axis=1).astype(bf16)
    for g in range(groups):
        old_re = state[pl.ds(g, R, stride=groups), :]
        old_im = state[pl.ds(R * groups + g, R, stride=groups), :]
        straight = jnp.concatenate([old_re, old_im], axis=1)
        swapped = jnp.concatenate([old_im, old_re], axis=1)
        moved[:, pl.ds(g * 2 * pst, 2 * pst)] = (
            coef[0, g:g + 1, :] * straight + coef[1, g:g + 1, :] * swapped
        )
    projected = jnp.dot(xv[...], w_in[...], preferred_element_type=f32).astype(bf16)
    scores = rw[...]
    scores = scores / jnp.sum(scores, axis=0, keepdims=True) * route_scale
    expert = lax.broadcasted_iota(jnp.int32, (experts, R), 0)
    table = jnp.zeros((experts, R), f32)
    for k in range(top_k):
        table += jnp.where(ids[k:k + 1, :] == expert, scores[k:k + 1, :], 0.0)
    for o in range(n_ep):
        wsend[o, pl.ds(0, local_experts), pl.ds(0, R)] = table[
            o * local_experts:(o + 1) * local_experts
        ]
    wrecv[e] = wsend[e]
    responses = []
    for h in range(lumps):
        pushed = jnp.dot(
            projected[:, h * 128:(h + 1) * 128], push[h], preferred_element_type=f32
        )
        fresh = []
        for k in range(lump):
            g = h * lump + k
            lanes = pl.ds(g * 2 * pst, 2 * pst)
            straight = pushed[:, k * 2 * pst:(k + 1) * 2 * pst]
            swapped = pltpu.roll(straight, pst, 1)
            new = moved[:, lanes] + (
                coef[2, g:g + 1, :] * straight + coef[3, g:g + 1, :] * swapped
            )
            kept[:, lanes] = new
            fresh.append(new)
        fresh = jnp.concatenate(fresh, axis=1).astype(bf16)
        responses.append(lax.dot_general(fresh, pull[h], NT, preferred_element_type=f32))
    response = jnp.concatenate(responses, axis=1) + skip_row * projected.astype(f32)
    act[t] = jax.nn.gelu(response).astype(bf16)
    pl.semaphore_wait(barrier, n_ep)
    swap = remote(act.at[t], act.at[t], act_s, act_r, {"tp": 1 - t})
    swap.start()

    @pl.loop(1, n_ep)
    def _(k):
        route((e + k) % n_ep).start()

    loads_a[13].wait()
    logits = jnp.dot(
        act[t], glu[pl.ds(pl.multiple_of(t * chans, chans), chans), :],
        preferred_element_type=f32,
    )
    loads_a[14].wait()
    loads_a[11].wait()
    loads_a[12].wait()
    remote(act.at[1 - t], act.at[1 - t], act_s, act_r, {"tp": 1 - t}).wait_recv()
    logits += jnp.dot(
        act[1 - t], glu[pl.ds(pl.multiple_of((1 - t) * chans, chans), chans), :],
        preferred_element_type=f32,
    )
    every = jnp.concatenate([act[0], act[1]], axis=1)
    glu_out = (every.astype(f32) * jax.nn.sigmoid(logits)).astype(bf16)
    mixed = jnp.dot(glu_out, mix[...], preferred_element_type=f32).astype(bf16)
    values = residual_alpha * xv[...].astype(f32) + mixed.astype(f32)
    values = values - jnp.mean(values, axis=1, keepdims=True)
    variance = jnp.mean(jnp.square(values), axis=1, keepdims=True)
    nrm[...] = (values * lax.rsqrt(variance + norm_eps) * ngain[...] + nshift[...]).astype(bf16)
    rows[t, z, a, b] = nrm[:, mine]

    @pl.loop(1, nz)
    def _(s):
        line_copy(event(s)).start()

    one(z, b).start()
    twoa(z).start()

    def shared():
        for g in range(groups):
            at = g * 2 * pst
            new_state[pl.ds(g, R, stride=groups), :] = kept[:, at:at + pst]
            new_state[pl.ds(R * groups + g, R, stride=groups), :] = kept[
                :, at + pst:at + 2 * pst
            ]
        for c in loads_b:
            c.wait()
        gu = jnp.dot(nrm[...], sgu[...], preferred_element_type=f32)
        sh = (jax.nn.silu(gu[:, :hid]) * gu[:, hid:]).astype(bf16)
        sh_own[...] = jnp.dot(sh, sd[:, mine], preferred_element_type=f32)
        sh_oth[...] = jnp.dot(sh, sd[:, peers], preferred_element_type=f32)
        gate = bgate[...].astype(f32)
        gate = jnp.concatenate([gate[k:k + 1] for k in range(gate.shape[0])], axis=1)
        din[pl.ds(dense_hid, 1), :] = gate.astype(bf16)

    blocks = [(k // 2, k % 2) for k in range(4)]

    def near_half(s, j):
        mine_x = jnp.concatenate([rows[t, j, aa, bb] for aa, bb in blocks], axis=0)
        for l in range(local_experts):
            gacc[s % 2, l] = jnp.dot(mine_x, wgu[l, mine, :], preferred_element_type=f32)
        dacc[s % 2] = lax.dot_general(mine_x, din[:, mine], NT, preferred_element_type=f32)

    def far_half(s, j):
        d_wait(j)
        if s == 0:
            routes().wait_recv()
        peer_x = jnp.concatenate([rows[1 - t, j, bb, aa] for aa, bb in blocks], axis=0)
        oth_part = None
        for l in range(local_experts):
            w = jnp.concatenate(
                [
                    column(
                        wrecv[
                            j * 4 + (aa * (1 - t) + bb * t) * 2 + bb * (1 - t) + aa * t,
                            l:l + 1, 0:R,
                        ],
                        R,
                    )
                    for aa, bb in blocks
                ],
                axis=0,
            )
            g = gacc[s % 2, l] + jnp.dot(peer_x, wgu[l, peers, :], preferred_element_type=f32)
            h = (jax.nn.silu(g[:, :ffn]) * g[:, ffn:] * w).astype(bf16)
            hbuf[s % 2, l] = h
            o = jnp.dot(h, wd[l, :, peers], preferred_element_type=f32)
            oth_part = o if oth_part is None else oth_part + o
        oth_part = oth_part.astype(bf16).reshape(4, R, half)
        for k, (aa, bb) in enumerate(blocks):
            pbuf[j, bb, aa] = oth_part[k]

        if s == 0:
            pbuf[j, b, a] = (pbuf[j, b, a].astype(f32) + sh_oth[...]).astype(bf16)
        part(j).start()

    def down(s, j):
        peer_x = jnp.concatenate([rows[1 - t, j, bb, aa] for aa, bb in blocks], axis=0)
        d = dacc[s % 2] + lax.dot_general(
            peer_x, din[:, peers], NT, preferred_element_type=f32
        )
        branch = jax.nn.sigmoid(d[:, dense_hid:dense_hid + 1])
        dh = (jax.nn.gelu(d[:, :dense_hid]) * branch).astype(bf16)
        own_part = jnp.dot(dh, dout[...], preferred_element_type=f32)
        for l in range(local_experts):
            own_part += jnp.dot(hbuf[s % 2, l], wd[l, :, mine], preferred_element_type=f32)
        own[j] = own_part.reshape(2, 2, R, half)

    def stage_a(s, j):
        line_wait(j)
        one(j, b).start()

    def stage_t(s, j):
        twoa(j).start()

    def stage_b(s, j):
        one(j, 1 - b).wait_recv()
        twob(j).start()
        da(j).start()

    def stage_c(s, j):
        two_wait(j)
        db(j).start()

    def stage_e(s, j):
        part(j).wait_recv()
        comb[j] = (own[j] + precv[j].astype(f32)).astype(bf16)
        firstx(j).start()

    def stage_y(s, j):
        firsty(j).start()

    def stage_f(s, j):
        firstx(j).wait_recv()
        s2buf[j] = (comb[j, a, 1 - b].astype(f32) + rs1[j, 1 - b].astype(f32)).astype(bf16)
        second(j).start()

    def stage_g(s, j):
        g_wait(j)
        summed = comb[j, a, b].astype(f32) + rs1[j, b].astype(f32) + rs2[j].astype(f32)

        if s == 0:
            acc[...] = summed + sh_own[...] + residual_alpha * nrm[:, mine].astype(f32)
        else:
            t3buf[j] = summed.astype(bf16)
            third(j).start()

    runs = dict(
        A=stage_a, B=stage_b, C=stage_c, P=near_half, Q=far_half, R=down, E=stage_e, F=stage_f,
        G=stage_g, T=stage_t, Y=stage_y,
    )
    extra = [name + str(j) for j in range(4, nz) for name in "ATBCPQREYFG"]
    for item in list(order) + extra:
        if item == "H":
            shared()
        else:
            s = int(item[1:])
            runs[item[0]](s, event(s))

    thirds().wait_recv()
    total = acc[...]
    for s in range(1, nz):
        total += t3recv[event(s)].astype(f32)
    lane = lax.broadcasted_iota(jnp.int32, stat.shape, 1)
    row_sum = jnp.sum(total, axis=1, keepdims=True)
    row_sq = jnp.sum(total * total, axis=1, keepdims=True)
    stat[...] = jnp.where(lane == 0, row_sum, row_sq)
    exchange = remote(stat, statr, stat_s, stat_r, {"tp": 1 - t})
    exchange.start()
    swap.wait_send()

    routes().wait_send()

    sent(rows, one_s)
    sent(rows.at[0, :, 0], db_s)
    sent(pbuf, p_s)
    sent(rows.at[0, lines, 0, 0], line_s)
    thirds().wait_send()
    exchange.wait()
    mean = (row_sum + statr[:, 0:1]) / width
    variance = (row_sq + statr[:, 1:2]) / width - mean * mean
    out[...] = (
        (total - mean) * lax.rsqrt(variance + norm_eps) * fnorm[0:1] + fnorm[1:2]
    ).astype(bf16)


def write_kernel(layer_v, state_v, layer_o, state_o, sems):
    copies = [
        pltpu.make_async_copy(state_v, state_o, sems.at[0]),
        pltpu.make_async_copy(layer_v, layer_o, sems.at[1]),
    ]
    for c in copies:
        c.start()
    for c in copies:
        c.wait()


def body(
    layer_input, ssm_state, w_input, decay_rate, frequency, step_log, input_map, output_map,
    skip_gain, glu_weight, mix_out, norm_gain, norm_shift, route_ids, route_weights,
    gate_expert, up_expert, down_expert, gate_shared, up_shared, down_shared,
    dense_in, dense_out, branch_gate, final_gain, final_shift,
):
    n_ep = lax.axis_size("ep")
    R, width = layer_input.shape
    half = width // 2
    local_experts, _, ffn = gate_expert.shape
    hid = gate_shared.shape[1]
    dense_hid = dense_in.shape[0]
    groups, gch = skip_gain.shape
    pst = decay_rate.shape[1]
    chans = groups * gch
    top_k = route_ids.shape[1]
    nz = n_ep // 4
    lumps = chans // 128
    wide = (128 // gch) * 2 * pst
    dense_pad = -(-(dense_hid + 1) // 128) * 128
    exp_pad = -(-local_experts // 8) * 8
    operands = (
        layer_input,
        ssm_state.reshape(2 * R * groups, pst),
        w_input,
        decay_rate,
        frequency,
        step_log[None, :],
        input_map.transpose(0, 1, 3, 2).reshape(2, chans, pst),
        output_map.reshape(2, chans, pst),
        skip_gain,
        glu_weight,
        mix_out,
        norm_gain[None, :],
        norm_shift[None, :],
        route_ids.T,
        route_weights.T,
        gate_expert, up_expert, down_expert, gate_shared, up_shared, down_shared,
        dense_in, dense_out,
        branch_gate.reshape(width // 128, 128),
        final_gain[None, :],
        final_shift[None, :],
    )
    hbm = pl.BlockSpec(memory_space=pl.ANY)
    vmem = pl.BlockSpec(memory_space=pltpu.VMEM)
    dma = pltpu.SemaphoreType.DMA

    def like(i):
        return pltpu.VMEM(operands[i].shape, operands[i].dtype)

    layer_output, new_state = pl.pallas_call(
        functools.partial(layer_kernel, n_ep, local_experts),
        out_shape=(
            pltpu.VMEM((R, half), bf16),
            pltpu.VMEM((2 * R * groups, pst), f32),
        ),
        in_specs=[hbm] * len(operands),
        out_specs=(vmem, vmem),
        scratch_shapes=[like(i) for i in range(15)]
        + [like(23), pltpu.VMEM((2, half), f32)]
        + [
            pltpu.VMEM((lumps, 128, wide), bf16),
            pltpu.VMEM((lumps, 128, wide), bf16),
            pltpu.VMEM((4, groups, 2 * pst), f32),
            pltpu.VMEM((R, groups * 2 * pst), f32),
            pltpu.VMEM((R, groups * 2 * pst), f32),
            pltpu.VMEM((2, R, chans), bf16),
            pltpu.VMEM((R, width), bf16),
            pltpu.VMEM((n_ep, exp_pad, 128), f32),
            pltpu.VMEM((n_ep, exp_pad, 128), f32),
            pltpu.VMEM((2, nz, 2, 2, R, half), bf16),
            pltpu.VMEM((local_experts, width, 2 * ffn), bf16),
            pltpu.VMEM((local_experts, ffn, width), bf16),
            pltpu.VMEM((width, 2 * hid), bf16),
            pltpu.VMEM((hid, width), bf16),
            pltpu.VMEM((dense_pad, width), bf16),
            pltpu.VMEM((dense_hid, half), bf16),
            pltpu.VMEM((nz, 2, 2, R, half), f32),
            pltpu.VMEM((2, local_experts, 4 * R, 2 * ffn), f32),
            pltpu.VMEM((2, 4 * R, dense_pad), f32),
            pltpu.VMEM((2, local_experts, 4 * R, ffn), bf16),
            pltpu.VMEM((nz, 2, 2, R, half), bf16),
            pltpu.VMEM((nz, 2, 2, R, half), bf16),
            pltpu.VMEM((nz, 2, 2, R, half), bf16),
            pltpu.VMEM((nz, 2, R, half), bf16),
            pltpu.VMEM((nz, R, half), bf16),
            pltpu.VMEM((nz, R, half), bf16),
            pltpu.VMEM((nz, R, half), bf16),
            pltpu.VMEM((nz, R, half), bf16),
            pltpu.VMEM((R, half), f32),
            pltpu.VMEM((R, half), f32),
            pltpu.VMEM((R, half), f32),
            pltpu.VMEM((R, 128), f32),
            pltpu.VMEM((R, 128), f32),
            dma((3,)),
            dma,
            dma,
            dma,
        ]
        + [dma((nz,))] * 7
        + [dma] * 10,
        compiler_params=pltpu.CompilerParams(
            collective_id=0, has_side_effects=True, vmem_limit_bytes=60 * 1024 * 1024
        ),
    )(*operands)
    layer_output, new_state = pl.pallas_call(
        write_kernel,
        out_shape=(
            jax.ShapeDtypeStruct((R, half), bf16),
            jax.ShapeDtypeStruct((2 * R * groups, pst), f32),
        ),
        in_specs=[vmem, vmem],
        out_specs=(hbm, hbm),
        scratch_shapes=[dma((2,))],
    )(
        pltpu.with_memory_space_constraint(layer_output, pltpu.VMEM),
        pltpu.with_memory_space_constraint(new_state, pltpu.VMEM),
    )
    return (layer_output, new_state.reshape(2, R, groups, pst))


def solution(mesh):
    placed = (
        P(("grp", "ep"), None),
        P(None, ("grp", "ep"), "tp", None),
        P(None, "tp"),
        P("tp", None),
        P("tp", None),
        P("tp"),
        P(None, "tp", None, None),
        P(None, "tp", None, None),
        P("tp", None),
        P(),
        P(),
        P(),
        P(),
        P(("grp", "ep"), None),
        P(("grp", "ep"), None),
        P("ep", None, "tp"),
        P("ep", None, "tp"),
        P("ep", "tp", None),
        P(None, "tp"),
        P(None, "tp"),
        P("tp", None),
        P("ep", None),
        P("ep", "tp"),
        P(),
        P("tp"),
        P("tp"),
    )
    return jax.shard_map(
        body,
        mesh=mesh,
        in_specs=placed,
        out_specs=(P(("grp", "ep"), "tp"), P(None, ("grp", "ep"), "tp", None)),
        check_vma=False,
    )
```
